32 devices in a mesh: sp: 4 (over z), fs: 4 (over y, x), tp: 2 (over core).
Axes of the slice: x: 2, y: 2, z: 4, core: 2. Of those that a mesh axis runs over, the one named last changes fastest.
Arguments:
- tokens: bfloat16 [4, 3072, 2048], P('fs', 'sp', 'tp'), may hold values from -6 to 6
- in_gain: float32 [2048], replicated, may hold values from 0.1 to 1.9
- ret_query: bfloat16 [2048, 768], P(None, 'tp'), may hold values from -0.125 to 0.125
- ret_key: bfloat16 [2048, 768], P(None, 'tp'), may hold values from -0.125 to 0.125
- ret_value: bfloat16 [2048, 768], P(None, 'tp'), may hold values from -0.125 to 0.125
- att_query: bfloat16 [2048, 768], P(None, 'tp'), may hold values from -8 to 8
- att_key: bfloat16 [2048, 256], P(None, 'tp'), may hold values from -8 to 8
- att_value: bfloat16 [2048, 256], P(None, 'tp'), may hold values from -0.125 to 0.125
- log_decay: float32 [4, 12, 3072], P('fs', 'tp', 'sp'), may hold values from -1.5 to 0
- ret_gain: float32 [768], P('tp'), may hold values from 0.1 to 1.9
- sink_logit: float32 [12], P('tp'), may hold values from 1 to 5
- retentive_exit_matrix: bfloat16 [768, 2048], P('tp'), may hold values from -0.15625 to 0.15625
- out_att: bfloat16 [768, 2048], P('tp'), may hold values from -0.875 to 0.875
Outputs:
- mixed: bfloat16 [4, 3072, 2048], P('fs', ('sp', 'tp'))
The draws below stay inside these ranges and needn't reach their ends.
All inputs are finite; a program needn't handle non-finite values.
Results may differ from the reference program's by a relative error of at most 0.0085.
Values may be sent and summed in bfloat16 or wider, within the bound.
A program may use at most 128 MiB of HBM per device.

```python
import jax
import jax.numpy as jnp
from jax import lax

D = 2048
HEAD_DIM = 64
RET_HEADS = 12
ATT_HEADS = 12
KV_HEADS = 4
WINDOW = 128
TOK_DEV = 768
SEQ = 3072
BATCH = 4


def paired_heads(key):
    keys = jax.random.split(jax.random.fold_in(key, 5), 2)
    key_weight = jax.random.normal(keys[0], (D, KV_HEADS * HEAD_DIM), jnp.float32) * D ** (-0.5)
    query_weight = jax.random.normal(keys[1], (D, ATT_HEADS * HEAD_DIM), jnp.float32) * D ** (-0.5)
    return (jnp.clip(query_weight, -8.0, 8.0), jnp.clip(key_weight, -8.0, 8.0))


def draw_att_query(key, part):
    return paired_heads(key)[0].astype(jnp.bfloat16)


def draw_att_key(key, part):
    return paired_heads(key)[1].astype(jnp.bfloat16)


def draw_log_decay(key, part):
    keys = jax.random.split(jax.random.fold_in(key, 11), 5)
    keep_share = 0.5
    slow = jax.random.uniform(keys[0], (BATCH, RET_HEADS, 1), jnp.float32) < keep_share
    span = 30.0 * jnp.exp(jax.random.uniform(keys[1], (BATCH, RET_HEADS, 1), jnp.float32) * jnp.log(100.0 / 30.0))
    starting_shift_amount = jnp.where(slow, -jnp.log(10.0) / (4.0 * SEQ), -1.0 / span)
    blocks = SEQ // TOK_DEV
    fading_multiplier = jnp.exp(jax.random.uniform(keys[2], (BATCH, 1, blocks), jnp.float32) * jnp.log(3.0))
    fading_multiplier = jnp.repeat(fading_multiplier, TOK_DEV, axis=2)
    location_numbers = jax.random.randint(keys[3], (BATCH, 3, 1), 0, SEQ)
    objective_numbers = jnp.log(1.0 - jax.random.uniform(keys[4], (BATCH, 3, 1), jnp.float32, 0.2, 0.5))
    element_locations = jnp.arange(SEQ)[None, None, :]
    cluster_sets = jnp.sum(jnp.where(element_locations == location_numbers, objective_numbers, 0.0), axis=1, keepdims=True)
    return (starting_shift_amount * fading_multiplier + cluster_sets).astype(jnp.float32)


def block_scale(key, dims, cuts, least, largest):
    def one(axis_at, shards_of):
        heights = jax.random.uniform(jax.random.fold_in(jax.random.fold_in(key, 6), axis_at), (shards_of,), jnp.float32, least / len(cuts), largest / len(cuts))
        return jnp.repeat(jnp.exp(heights), dims[axis_at] // shards_of).reshape((-1,) + (1,) * (len(dims) - axis_at - 1))

    level = one(*cuts[0])
    for cut in cuts[1:]:
        level = level * one(*cut)
    return level


def gaussian(key, dims, width, reach, pieces=(), held_as=jnp.bfloat16):
    array = jax.random.normal(key, dims, jnp.float32) * width
    if len(pieces) > 0:
        array = block_scale(key, dims, pieces, -0.22, 0.18) * array
    return jnp.clip(array, min=-reach, max=reach).astype(held_as)


def setup_inputs(seed: int = 0) -> dict:
    arg_keys = jax.random.split(jax.random.key(seed), 14)
    tokens = gaussian(arg_keys[0], (BATCH, SEQ, D), 1.0, 6.0, ((0, 4), (1, 4), (2, 2)))
    in_gain = jnp.clip(1.0 + 0.18 * jax.random.normal(arg_keys[1], (D,), jnp.float32), 0.1, 1.9)
    ret_query = gaussian(arg_keys[2], (D, RET_HEADS * HEAD_DIM), D ** -0.5, 0.125, ((1, 2),))
    ret_key = gaussian(arg_keys[3], (D, RET_HEADS * HEAD_DIM), D ** -0.5, 0.125, ((1, 2),))
    ret_value = gaussian(arg_keys[4], (D, RET_HEADS * HEAD_DIM), D ** -0.5, 0.125, ((1, 2),))
    att_query = draw_att_query(jax.random.fold_in(arg_keys[13], 71), 0)
    att_key = draw_att_key(jax.random.fold_in(arg_keys[13], 71), 0)
    att_value = gaussian(arg_keys[7], (D, KV_HEADS * HEAD_DIM), D ** -0.5, 0.125, ((1, 2),))
    log_decay = draw_log_decay(jax.random.fold_in(arg_keys[13], 71), 0)
    ret_gain = jnp.clip(1.0 + 0.18 * jax.random.normal(arg_keys[9], (RET_HEADS * HEAD_DIM,), jnp.float32), 0.1, 1.9)
    sink_logit = jnp.clip(1.0 + 4.0 * jax.random.uniform(arg_keys[10], (ATT_HEADS,), jnp.float32) ** block_scale(arg_keys[10], (ATT_HEADS,), ((0, 2),), -0.2, 0.2), 1.0, 5.0)
    retentive_exit_matrix = gaussian(arg_keys[11], (RET_HEADS * HEAD_DIM, D), (2 * RET_HEADS * HEAD_DIM) ** -0.5, 0.15625, ((0, 2),))
    out_att = gaussian(arg_keys[12], (ATT_HEADS * HEAD_DIM, D), (ATT_HEADS * HEAD_DIM // 16) ** -0.5, 0.875, ((0, 2),))
    return dict(tokens=tokens, in_gain=in_gain, ret_query=ret_query, ret_key=ret_key, ret_value=ret_value, att_query=att_query, att_key=att_key, att_value=att_value, log_decay=log_decay, ret_gain=ret_gain, sink_logit=sink_logit, retentive_exit_matrix=retentive_exit_matrix, out_att=out_att)


EPS = 1e-06

def retention_sequence(query_rows, key_rows, value_rows, log_rates, gain):
    heads = log_rates.shape[0]
    blocks = query_rows.shape[0] // TOK_DEV
    fading_multiplier = HEAD_DIM ** (-0.5)
    shaped_q = query_rows.reshape(blocks, TOK_DEV, heads, HEAD_DIM)
    shaped_k = key_rows.reshape(blocks, TOK_DEV, heads, HEAD_DIM)
    shaped_v = value_rows.reshape(blocks, TOK_DEV, heads, HEAD_DIM)
    shaped_r = log_rates.reshape(heads, blocks, TOK_DEV).transpose(1, 0, 2)
    later = jnp.arange(TOK_DEV)[:, None] >= jnp.arange(TOK_DEV)[None, :]

    def advance(state, inputs):
        block_q, block_k, block_v, block_r = inputs
        cumulative = jnp.cumsum(block_r, axis=1)
        decay = jnp.exp(jnp.where(later[None], cumulative[:, :, None] - cumulative[:, None, :], -jnp.inf))
        query_f = block_q.astype(jnp.float32)
        key_f = block_k.astype(jnp.float32)
        value_f = block_v.astype(jnp.float32)
        weights = (jnp.einsum('thd,shd->hts', query_f, key_f) * fading_multiplier * decay).astype(jnp.bfloat16)
        inner = jnp.einsum('hts,shd->thd', weights.astype(jnp.float32), value_f)
        carried = jnp.einsum('thd,hde->the', query_f, state, precision=lax.Precision.HIGHEST)
        carried = carried * jnp.exp(cumulative).T[:, :, None]
        keyed = key_f * (jnp.exp(cumulative[:, -1:] - cumulative) * fading_multiplier).T[:, :, None]
        own_state = jnp.einsum('shd,she->hde', keyed, value_f, precision=lax.Precision.HIGHEST)
        state = jnp.exp(cumulative[:, -1])[:, None, None] * state + own_state
        return (state, inner + carried)
    start_state = jnp.zeros((heads, HEAD_DIM, HEAD_DIM), jnp.float32)
    _, outputs = lax.scan(advance, start_state, (shaped_q, shaped_k, shaped_v, shaped_r))
    outputs = outputs.reshape(-1, heads, HEAD_DIM)
    normed = outputs * lax.rsqrt(lax.optimization_barrier(jnp.mean(outputs * outputs, axis=-1, keepdims=True)) + EPS)
    return (normed.reshape(-1, heads * HEAD_DIM) * gain).astype(jnp.bfloat16)

def window_attention(query_rows, key_ext, value_ext, first_position, sinks):
    length = query_rows.shape[0]
    blocks = length // WINDOW
    heads_kv = key_ext.shape[1] // HEAD_DIM
    heads = query_rows.shape[1] // HEAD_DIM
    group = heads // heads_kv
    shaped_q = query_rows.astype(jnp.float32).reshape(blocks, WINDOW, heads_kv, group, HEAD_DIM)
    key_block_list = key_ext.astype(jnp.float32).reshape(blocks + 1, WINDOW, heads_kv, HEAD_DIM)
    value_blocks = value_ext.astype(jnp.float32).reshape(blocks + 1, WINDOW, heads_kv, HEAD_DIM)
    key_band = jnp.concatenate([key_block_list[:-1], key_block_list[1:]], axis=1)
    value_band = jnp.concatenate([value_blocks[:-1], value_blocks[1:]], axis=1)
    scores = jnp.einsum('nqhgd,nkhd->hgnqk', shaped_q, key_band) * HEAD_DIM ** (-0.5)
    distance = WINDOW + jnp.arange(WINDOW)[:, None] - jnp.arange(2 * WINDOW)[None, :]
    key_position = first_position - WINDOW + jnp.arange(blocks)[:, None] * WINDOW + jnp.arange(2 * WINDOW)[None, :]
    allowed = ((distance >= 0) & (distance < WINDOW))[None] & (key_position >= 0)[:, None, :]
    scores = jnp.where(allowed, scores, -jnp.inf)
    sink_part = sinks.reshape(heads_kv, group, 1, 1, 1)
    greatest_level = jnp.maximum(lax.optimization_barrier(jnp.max(scores, axis=-1, keepdims=True)), sink_part)
    raised = jnp.exp(scores - greatest_level)
    totals = lax.optimization_barrier(jnp.sum(raised, axis=-1, keepdims=True)) + jnp.exp(sink_part - greatest_level)
    weights = (raised / totals).astype(jnp.bfloat16)
    outputs = jnp.einsum('hgnqk,nkhd->nqhgd', weights.astype(jnp.float32), value_band)
    return outputs.reshape(length, heads * HEAD_DIM).astype(jnp.bfloat16)

def reference(tokens, in_gain, ret_query, ret_key, ret_value, att_query, att_key, att_value, log_decay, ret_gain, sink_logit, retentive_exit_matrix, out_att):
    results = []
    for sequence in range(tokens.shape[0]):
        wide = tokens[sequence].astype(jnp.float32)
        inverse = lax.rsqrt(lax.optimization_barrier(jnp.mean(wide * wide, axis=-1, keepdims=True)) + EPS)
        scaled = (wide * in_gain).astype(jnp.bfloat16)

        def project(weight):
            return (jnp.dot(scaled, weight, preferred_element_type=jnp.float32) * inverse).astype(jnp.bfloat16)
        ret_q = project(ret_query)
        ret_k = project(ret_key)
        ret_v = project(ret_value)
        att_q = project(att_query)
        att_k = project(att_key)
        att_v = project(att_value)
        ret_out = retention_sequence(ret_q, ret_k, ret_v, log_decay[sequence], ret_gain)
        padding = jnp.zeros((WINDOW, att_k.shape[1]), jnp.bfloat16)
        att_out = window_attention(att_q, jnp.concatenate([padding, att_k], axis=0), jnp.concatenate([padding, att_v], axis=0), 0, sink_logit)
        summed = jnp.dot(ret_out, retentive_exit_matrix, preferred_element_type=jnp.float32) + jnp.dot(att_out, out_att, preferred_element_type=jnp.float32)
        results.append(summed.astype(jnp.bfloat16))
    return jnp.stack(results)
```

```python
import functools

import jax
import jax.numpy as jnp
from jax import lax
from jax.experimental import pallas as pl
from jax.experimental.pallas import tpu as pltpu
from jax.sharding import PartitionSpec as P

HEAD_DIM = 64
WINDOW = 128
CHUNK = 128
LANES = 128
TILE = 256
EPS = 1e-06
F32 = jnp.float32
BF16 = jnp.bfloat16

NT = (((1,), (1,)), ((), ()))
TN = (((0,), (0,)), ((), ()))


def weave(*streams):
    order = []
    for k, stream in enumerate(streams):
        for i, piece in enumerate(stream):
            order.append(((i + 0.5) / len(stream), k, i, piece))
    for item in sorted(order, key=lambda entry: entry[:3]):
        item[3]()


def layer(
    n_sp, n_tp,
    tok, gain_in, rq, rk, rv, aq, ak, av, ld_in, rgain_in, sink_in, wr, wa,
    out,
    xb, wb, acc, pb, sq, inv, cr, eqr, ekr, dt, vt, ub, st, stb, ri, bias, sc, pw, dn,
    msg, inbox, hb, hin, wo, oacc, gt,
    gain, ld, rgain, sink, small_sem, tok_sem, w_sem, wo_sem, x_send, x_recv, wo_send, wo_recv,
    h_send, h_recv, m_send, m_recv, halo_send, halo_recv,
):
    tp = lax.axis_index("tp")
    sp = lax.axis_index("sp")
    rows, depth = tok.shape
    ret_w, att_w, kv_w = rq.shape[1], aq.shape[1], ak.shape[1]
    heads = ld_in.shape[0]
    chunks = rows // CHUNK
    pairs = ret_w // LANES
    att_pairs = att_w // LANES
    att_heads = att_w // HEAD_DIM
    kv_heads = kv_w // HEAD_DIM
    group = att_heads // kv_heads
    out_rows = rows // n_tp
    model = depth * n_tp
    scale = HEAD_DIM ** (-0.5)
    half = rows // 2
    blocks = rows // WINDOW

    c_rk, c_rv, c_ak = 0, ret_w, 2 * ret_w
    c_av = c_ak + kv_w
    c_rq = c_av + kv_w
    c_aq = c_rq + ret_w
    width = c_aq + att_w
    parts = ((rk, c_rk), (rv, c_rv), (ak, c_ak), (av, c_av), (rq, c_rq), (aq, c_aq))
    tiles = width // TILE
    ret_tiles = c_ak // TILE
    kv_tiles = c_rq // TILE

    def load_tokens(i):
        span = pl.ds(i * half, half)
        return pltpu.make_async_copy(tok.at[span, :], xb.at[0, span, :], tok_sem.at[i])

    def load_weight(phase, i):
        owner = lax.rem(tp + phase, n_tp)
        ref, col = parts[i]
        return pltpu.make_async_copy(
            ref.at[pl.ds(owner * depth, depth), :],
            wb.at[phase, :, pl.ds(col, ref.shape[1])],
            w_sem.at[phase, i],
        )

    def load_exit(i):
        ref = (wr, wa)[i]
        return pltpu.make_async_copy(
            ref, wo.at[i, pl.ds(0, ref.shape[0]), :], wo_sem.at[i]
        )

    def send_tokens(q, i):
        span = pl.ds(i * half, half)
        return pltpu.make_async_remote_copy(
            src_ref=tok.at[span, :], dst_ref=xb.at[n_tp - q, span, :],
            send_sem=x_send.at[q - 1, i], recv_sem=x_recv.at[n_tp - q - 1, i],
            device_id={"tp": lax.rem(tp + q, n_tp)}, device_id_type=pl.DeviceIdType.MESH,
        )

    def send_exit(q, i):
        ref = (wr, wa)[i]
        return pltpu.make_async_remote_copy(
            src_ref=ref,
            dst_ref=wo.at[i, pl.ds((n_tp - q) * ref.shape[0], ref.shape[0]), :],
            send_sem=wo_send.at[q - 1, i], recv_sem=wo_recv.at[n_tp - q - 1, i],
            device_id={"tp": lax.rem(tp + q, n_tp)}, device_id_type=pl.DeviceIdType.MESH,
        )

    def send_heads(q, i):
        target = lax.rem(tp + q, n_tp)
        cols = pl.ds(i * ret_w, (ret_w, att_w)[i])
        return pltpu.make_async_remote_copy(
            src_ref=hb.at[pl.ds(target * out_rows, out_rows), cols],
            dst_ref=hin.at[n_tp - q - 1, :, cols],
            send_sem=h_send.at[q - 1, i], recv_sem=h_recv.at[n_tp - q - 1, i],
            device_id={"tp": target}, device_id_type=pl.DeviceIdType.MESH,
        )

    def send_state(q):
        return pltpu.make_async_remote_copy(
            src_ref=msg, dst_ref=inbox.at[q - 1],
            send_sem=m_send.at[q - 1], recv_sem=m_recv.at[q - 1],
            device_id={"sp": lax.rem(sp + q, n_sp)}, device_id_type=pl.DeviceIdType.MESH,
        )

    def send_halo():
        cols = pl.ds(c_ak, 2 * kv_w)
        return pltpu.make_async_remote_copy(
            src_ref=pb.at[pl.ds(rows, WINDOW), cols],
            dst_ref=pb.at[pl.ds(0, WINDOW), cols],
            send_sem=halo_send, recv_sem=halo_recv,
            device_id={"sp": lax.rem(sp + 1, n_sp)}, device_id_type=pl.DeviceIdType.MESH,
        )

    smalls = [
        pltpu.make_async_copy(src, dst, small_sem.at[i])
        for i, (src, dst) in enumerate(
            ((ld_in, ld), (gain_in, gain), (rgain_in, rgain), (sink_in, sink))
        )
    ]
    for copy in smalls:
        copy.start()
    for i in range(2):
        load_tokens(i).start()
    for i in range(2):
        load_weight(0, i).start()
    barrier = pltpu.get_barrier_semaphore()
    for q in range(1, n_tp):
        pl.semaphore_signal(
            barrier, inc=1, device_id={"tp": lax.rem(tp + q, n_tp)},
            device_id_type=pl.DeviceIdType.MESH,
        )
    for q in range(1, n_sp):
        pl.semaphore_signal(
            barrier, inc=1, device_id={"sp": lax.rem(sp + q, n_sp)},
            device_id_type=pl.DeviceIdType.MESH,
        )

    lane1 = lax.broadcasted_iota(jnp.int32, (1, LANES), 1)
    first_lanes = lane1 < HEAD_DIM
    half_masks = (
        jnp.where(first_lanes, scale, 0.0).astype(BF16),
        jnp.where(first_lanes, 0.0, scale).astype(BF16),
    )
    lane = lax.broadcasted_iota(jnp.int32, (CHUNK, LANES), 1)
    row = lax.broadcasted_iota(jnp.int32, (CHUNK, LANES), 0)
    same_head = (row < HEAD_DIM) == (lane < HEAD_DIM)
    k_at = lax.broadcasted_iota(jnp.int32, (2 * WINDOW, WINDOW), 0)
    q_at = lax.broadcasted_iota(jnp.int32, (2 * WINDOW, WINDOW), 1)
    in_window = (k_at > q_at) & (k_at <= q_at + WINDOW)
    bias[0] = jnp.where(in_window, 0.0, -jnp.inf)
    bias[1] = jnp.where(in_window & (k_at >= WINDOW), 0.0, -jnp.inf)

    pad = cr.shape[1]
    cr[...] = jnp.zeros_like(cr)
    for copy in smalls:
        copy.wait()
    for p in range(pairs):
        gt[p] = jnp.broadcast_to(
            rgain[p * LANES : (p + 1) * LANES].reshape(1, LANES), (LANES, LANES)
        ).T
    for h in range(heads):
        for c in range(chunks):
            cr[c, h : h + 1, :] = ld[h, :, c * CHUNK : (c + 1) * CHUNK]
    steps = cr[...].reshape(chunks * pad, CHUNK)
    top = steps.astype(BF16)
    rest = steps - top.astype(F32)
    mid = rest.astype(BF16)
    low = (rest - mid.astype(F32)).astype(BF16)
    upto = jnp.where(row <= lane, 1.0, 0.0).astype(BF16)
    sums = jnp.dot(
        jnp.concatenate([top, mid, low], axis=0), upto, preferred_element_type=F32
    )
    n_steps = chunks * pad
    cumulative = sums[:n_steps] + (sums[n_steps : 2 * n_steps] + sums[2 * n_steps :])
    cr[...] = cumulative.reshape(chunks, pad, CHUNK)
    eqr[...] = jnp.exp(cumulative).reshape(chunks, pad, CHUNK)
    ekr[...] = (jnp.exp(cumulative[:, CHUNK - 1 :] - cumulative) * scale).reshape(
        chunks, pad, CHUNK
    )
    filler = jnp.zeros((LANES - n_steps % LANES, CHUNK), F32)
    columns = jnp.concatenate([cumulative, filler], axis=0).T

    def decay(c, h):
        def piece():
            at = c * pad + h
            wide = jnp.broadcast_to(columns[:, at : at + 1], (CHUNK, LANES))
            gap = jnp.where(row <= lane, cr[c, h : h + 1, :] - wide, -jnp.inf)
            dt[c, h // 2, :, (h % 2) * CHUNK : (h % 2 + 1) * CHUNK] = jnp.exp(gap)

        return piece

    def scaled(phase, i):
        def piece():
            owner = lax.rem(tp + phase, n_tp)
            span = slice(i * CHUNK, (i + 1) * CHUNK)
            x = xb[phase, span, :].astype(F32)
            xb[phase, span, :] = (x * gain[owner]).astype(BF16)
            squares = jnp.broadcast_to(
                jnp.sum(x * x, axis=1, keepdims=True), (CHUNK, LANES)
            )
            if phase > 0:
                squares = sq[span, :] + squares
            if phase == n_tp - 1:
                inv[span, :] = lax.rsqrt(squares / model + EPS)
            else:
                sq[span, :] = squares

        return piece

    def project(phase, n, i, parts_of=2):
        def piece():
            size = rows // parts_of
            cols = slice(n * TILE, (n + 1) * TILE)
            span = slice(i * size, (i + 1) * size)
            total = jnp.dot(
                xb[phase, span, :], wb[phase, :, cols], preferred_element_type=F32
            )
            if phase > 0:
                total = acc[span, cols] + total
            if phase == n_tp - 1:
                wide = jnp.concatenate([inv[span, :]] * (TILE // LANES), axis=1)
                pb[WINDOW + i * size : WINDOW + (i + 1) * size, cols] = (
                    total * wide
                ).astype(BF16)
            else:
                acc[span, cols] = total

        return piece

    per_half = half // CHUNK
    load_tokens(0).wait()
    for i in range(2, 6):
        load_weight(0, i).start()
    weave([scaled(0, i) for i in range(per_half)])
    load_tokens(1).wait()
    for i in range(2):
        load_weight(0, i).wait()
    decays = [decay(c, h) for c in range(chunks) for h in range(heads)]
    weave(
        [project(0, n, 0) for n in range(ret_tiles)],
        [scaled(0, i) for i in range(per_half, chunks)],
    )
    cut = len(decays) // 2
    weave([project(0, n, 1) for n in range(ret_tiles)], decays[:cut])
    pl.semaphore_wait(barrier, n_tp - 1 + n_sp - 1)
    for q in range(1, n_tp):
        for i in range(2):
            send_tokens(q, i).start()
    for phase in range(1, n_tp):
        for i in range(6):
            load_weight(phase, i).start()
    for i in range(2, 6):
        load_weight(0, i).wait()
    weave([project(0, n, 0, 1) for n in range(ret_tiles, tiles)], decays[cut:])
    for q in range(1, n_tp):
        for i in range(1, -1, -1):
            send_exit(q, i).start()
    for i in range(1, -1, -1):
        load_exit(i).start()
    for phase in range(1, n_tp - 1):
        for i in range(2):
            send_tokens(n_tp - phase, i).wait_recv()
        for i in range(6):
            load_weight(phase, i).wait()
        weave([scaled(phase, i) for i in range(chunks)])
        weave([project(phase, n, 0, 1) for n in range(tiles)])
    last = n_tp - 1
    for i in range(6):
        load_weight(last, i).wait()
    send_tokens(n_tp - last, 0).wait_recv()
    weave([scaled(last, i) for i in range(per_half)])
    send_tokens(n_tp - last, 1).wait_recv()

    def here(c):
        return pl.ds(pl.multiple_of(WINDOW + c * CHUNK, CHUNK), CHUNK)

    def own_state(c):
        def piece():
            for p in range(pairs):
                cols = slice(c_rv + p * LANES, c_rv + (p + 1) * LANES)
                turned = pb[here(c), cols].T
                vt[c, p] = turned
                wide = turned.astype(F32)
                faded = jnp.concatenate(
                    [
                        wide[:HEAD_DIM] * ekr[c, 2 * p : 2 * p + 1, :],
                        wide[HEAD_DIM:] * ekr[c, 2 * p + 1 : 2 * p + 2, :],
                    ],
                    axis=0,
                ).astype(BF16)
                keys = pb[here(c), c_rk + p * LANES : c_rk + (p + 1) * LANES]
                added = jnp.dot(faded, keys, preferred_element_type=F32)
                ub[c, p] = jnp.where(same_head, added, 0.0)

        return piece

    def fade_row(c, p):
        ends = [
            jnp.broadcast_to(eqr[c, h : h + 1, CHUNK - 1 :], (1, LANES))
            for h in (2 * p, 2 * p + 1)
        ]
        return jnp.where(first_lanes, ends[0], ends[1])

    weave(
        [project(last, n, 0) for n in range(ret_tiles)],
        [scaled(last, i) for i in range(per_half, chunks)],
    )
    weave(
        [project(last, n, 1) for n in range(ret_tiles)],
        [own_state(c) for c in range(per_half)],
    )
    weave([own_state(c) for c in range(per_half, chunks)])
    totals = []
    for p in range(pairs):
        state = ub[0, p]
        total = fade_row(0, p)
        for c in range(1, chunks):
            fade = fade_row(c, p)
            state = state * fade + ub[c, p]
            total = total * fade
        msg[p * HEAD_DIM : (p + 1) * HEAD_DIM, :] = (
            state[:HEAD_DIM] + state[HEAD_DIM:]
        ).astype(BF16)
        coarse = total.astype(BF16).astype(F32)
        totals += [coarse, total - coarse]
    row16 = lax.broadcasted_iota(jnp.int32, (16, LANES), 0)
    tail = jnp.zeros((16, LANES), F32)
    for i, value in enumerate(totals):
        tail = jnp.where(row16 == i, value, tail)
    msg[pairs * HEAD_DIM :, :] = tail.astype(BF16)
    for q in range(n_sp - 1, 0, -1):
        @pl.when(sp + q < n_sp)
        def _():
            send_state(q).start()

    weave([project(last, n, 0, 1) for n in range(ret_tiles, kv_tiles)])

    @pl.when(sp + 1 < n_sp)
    def _():
        send_halo().start()

    weave([project(last, n, 0, 1) for n in range(tiles - 1, kv_tiles, -1)])

    def score(n):
        def piece(g):
            t, e = g // 2, g % 2
            band = pl.ds(n * WINDOW, 2 * WINDOW)
            keys = pb[band, c_ak + t * LANES : c_ak + (t + 1) * LANES]
            swapped = pltpu.roll(keys.astype(F32), HEAD_DIM, 1).astype(BF16)
            both = jnp.where(first_lanes == (e == 0), keys, swapped)
            queries = []
            for h in range(g * group, (g + 1) * group):
                at = c_aq + (h // 2) * LANES
                queries.append(pb[here(n), at : at + LANES] * half_masks[h % 2])
            sc[n, :, g * group * WINDOW : (g + 1) * group * WINDOW] = lax.dot_general(
                both, jnp.concatenate(queries, axis=0), NT, preferred_element_type=F32
            )

        return [functools.partial(piece, g) for g in range(kv_heads)]

    cut_off = jnp.where(sp == 0, 1, 0)
    step = 32

    def weigh(n):
        def piece(h):
            cols = slice(h * WINDOW, (h + 1) * WINDOW)
            masked = bias.at[cut_off if n == 0 else 0]
            tops = []
            for i in range(2 * WINDOW // step):
                span = slice(i * step, (i + 1) * step)
                s = sc[n, span, cols] + masked[span, :]
                tops.append(jnp.max(s, axis=0, keepdims=True))
            sink_h = jnp.full((1, WINDOW), sink[h], F32)
            top = functools.reduce(jnp.maximum, tops, sink_h)
            dn[n, h : h + 1, :] = jnp.exp(sink_h - top)
            for i in range(2 * WINDOW // step):
                span = slice(i * step, (i + 1) * step)
                s = sc[n, span, cols] + masked[span, :]
                pw[n, span, cols] = jnp.exp(s - top).astype(BF16)

        return [functools.partial(piece, h) for h in range(att_heads)]

    def gather(n):
        def piece():
            band = pl.ds(n * WINDOW, 2 * WINDOW)
            ones = jnp.ones((16, 2 * WINDOW), BF16)
            turned = [
                pb[band, c_av + t * LANES : c_av + (t + 1) * LANES].T
                for t in range(kv_w // LANES)
            ]
            parts_out = []
            for g in range(kv_heads):
                e = g % 2
                left = jnp.concatenate(
                    [turned[g // 2][e * HEAD_DIM : (e + 1) * HEAD_DIM], ones], axis=0
                )
                cols = slice(g * group * WINDOW, (g + 1) * group * WINDOW)
                total = jnp.dot(left, pw[n, :, cols], preferred_element_type=F32)
                for j in range(group):
                    h = g * group + j
                    cols = slice(j * WINDOW, (j + 1) * WINDOW)
                    below = total[HEAD_DIM : HEAD_DIM + 1, cols] + dn[n, h : h + 1, :]
                    parts_out.append((total[:HEAD_DIM, cols] * (1.0 / below)).astype(BF16))
            for p in range(att_pairs):
                hb[n * WINDOW : (n + 1) * WINDOW, ret_w + p * LANES : ret_w + (p + 1) * LANES] = (
                    jnp.concatenate(parts_out[2 * p : 2 * p + 2], axis=0).T
                )

        return [piece]

    order = list(range(blocks - 1, -1, -1))
    rest = [project(last, kv_tiles, i) for i in range(2)]
    for i in range(blocks + 2):
        if i == blocks - 1:
            @pl.when(sp > 0)
            def _():
                send_halo().wait_recv()

            @pl.when(sp == 0)
            def _():
                pb[:WINDOW, c_ak : c_ak + 2 * kv_w] = jnp.zeros((WINDOW, 2 * kv_w), BF16)
        weave(
            score(order[i]) if i < blocks else [],
            weigh(order[i - 1]) if 0 <= i - 1 < blocks else [],
            gather(order[i - 2]) if 0 <= i - 2 < blocks else [],
            [rest.pop()] if rest and i > 0 else [],
        )
    for q in range(1, n_tp):
        send_heads(q, 1).start()

    def intra(c):
        def piece(p):
            query = pb[here(c), c_rq + p * LANES : c_rq + (p + 1) * LANES]
            keys = pb[here(c), c_rk + p * LANES : c_rk + (p + 1) * LANES]
            queries = jnp.concatenate([query * half_masks[e] for e in range(2)], axis=0)
            weights = (
                lax.dot_general(keys, queries, NT, preferred_element_type=F32) * dt[c, p]
            ).astype(BF16)
            total = jnp.dot(vt[c, p], weights, preferred_element_type=F32)
            ri[c, p, :HEAD_DIM, :] = total[:HEAD_DIM, :CHUNK]
            ri[c, p, HEAD_DIM:, :] = total[HEAD_DIM:, CHUNK:]

        return [functools.partial(piece, p) for p in range(pairs)]

    weave([piece for c in range(chunks) for piece in intra(c)])

    st[...] = jnp.zeros_like(st)
    for q in range(n_sp - 1, 0, -1):
        @pl.when(sp >= q)
        def _():
            send_state(q).wait_recv()
            tail = inbox[q - 1, pairs * HEAD_DIM :, :].astype(F32)
            for p in range(pairs):
                part = inbox[q - 1, p * HEAD_DIM : (p + 1) * HEAD_DIM, :].astype(F32)
                fade = tail[2 * p : 2 * p + 1] + tail[2 * p + 1 : 2 * p + 2]
                both = jnp.concatenate([part, part], axis=0)
                st[p] = st[p] * fade + jnp.where(same_head, both, 0.0)

    for p in range(pairs):
        state = st[p]
        for c in range(chunks):
            stb[c, p] = state.astype(BF16)
            if c + 1 < chunks:
                state = state * fade_row(c, p) + ub[c, p]

    mine = pl.ds(pl.multiple_of(tp * out_rows, out_rows), out_rows)
    ranks = n_tp * ret_w

    def leave(kind, n):
        def piece():
            cols = slice(n * TILE, (n + 1) * TILE)
            inner = slice(kind * ret_w, (kind + 1) * ret_w)
            left = jnp.concatenate(
                [hb[mine, inner]] + [hin[phase - 1, :, inner] for phase in range(1, n_tp)],
                axis=1,
            )
            total = jnp.dot(left, wo[kind, :, cols], preferred_element_type=F32)
            if kind == 1:
                oacc[:, cols] = total
            else:
                out[:, cols] = (oacc[:, cols] + total).astype(BF16)

        return piece

    def finish(c):
        def piece(p):
            query = pb[here(c), c_rq + p * LANES : c_rq + (p + 1) * LANES]
            carried = lax.dot_general(stb[c, p], query, NT, preferred_element_type=F32)
            normed = []
            for e in range(2):
                span = slice(e * HEAD_DIM, (e + 1) * HEAD_DIM)
                h = 2 * p + e
                r = ri[c, p, span, :] + carried[span] * eqr[c, h : h + 1, :]
                square = jnp.sum(r * r, axis=0, keepdims=True)
                normed.append(
                    (r * lax.rsqrt(square * (1.0 / HEAD_DIM) + EPS) * gt[p, span, :]).astype(BF16)
                )
            rows_c = pl.ds(pl.multiple_of(c * CHUNK, CHUNK), CHUNK)
            hb[rows_c, p * LANES : (p + 1) * LANES] = jnp.concatenate(normed, axis=0).T

        return [functools.partial(piece, p) for p in range(pairs)]

    for i in range(2):
        load_exit(i).wait()
    for phase in range(1, n_tp):
        for i in range(2):
            send_exit(n_tp - phase, i).wait_recv()
        send_heads(n_tp - phase, 1).wait_recv()
    each = chunks // n_tp
    exits = [leave(1, n) for n in range(model // TILE)]
    share = len(exits) // n_tp
    for q in range(1, n_tp + 1):
        first = lax.rem(tp + q, n_tp) * each
        weave(
            [piece for i in range(each) for piece in finish(first + i)],
            exits[(q - 1) * share : q * share if q < n_tp else len(exits)],
        )
        if q < n_tp:
            send_heads(q, 0).start()
    for phase in range(1, n_tp):
        send_heads(n_tp - phase, 0).wait_recv()
    weave([leave(0, n) for n in range(model // TILE)])
    for q in range(1, n_tp):
        for i in range(2):
            send_tokens(q, i).wait_send()
            send_exit(q, i).wait_send()
            send_heads(q, i).wait_send()
    for q in range(1, n_sp):
        @pl.when(sp + q < n_sp)
        def _():
            send_state(q).wait_send()

    @pl.when(sp + 1 < n_sp)
    def _():
        send_halo().wait_send()


def shards(n_sp, n_tp, tokens, in_gain, rq, rk, rv, aq, ak, av, log_decay, ret_gain, sink, wr, wa):
    rows, depth = tokens.shape[1:]
    ret_w, att_w, kv_w = rq.shape[1], aq.shape[1], ak.shape[1]
    heads = log_decay.shape[1]
    model = depth * n_tp
    width = 3 * ret_w + att_w + 2 * kv_w
    chunks, pairs, blocks = rows // CHUNK, ret_w // LANES, rows // WINDOW
    att_heads = att_w // HEAD_DIM
    out_rows = rows // n_tp
    later = max(n_sp - 1, 1)
    others = max(n_tp - 1, 1)
    packed = pairs * HEAD_DIM + 16
    pad = 8
    hbm = pl.BlockSpec(memory_space=pltpu.HBM)
    dma = pltpu.SemaphoreType.DMA
    result = pl.pallas_call(
        functools.partial(layer, n_sp, n_tp),
        out_shape=pltpu.VMEM((out_rows, model), BF16),
        in_specs=[hbm] * 13,
        out_specs=pl.BlockSpec(memory_space=pltpu.VMEM),
        scratch_shapes=[
            pltpu.VMEM((n_tp, rows, depth), BF16),
            pltpu.VMEM((n_tp, depth, width), BF16),
            pltpu.VMEM((rows, width), F32),
            pltpu.VMEM((WINDOW + rows, width), BF16),
            pltpu.VMEM((rows, LANES), F32),
            pltpu.VMEM((rows, LANES), F32),
            pltpu.VMEM((chunks, pad, CHUNK), F32),
            pltpu.VMEM((chunks, pad, CHUNK), F32),
            pltpu.VMEM((chunks, pad, CHUNK), F32),
            pltpu.VMEM((chunks, pairs, CHUNK, 2 * CHUNK), F32),
            pltpu.VMEM((chunks, pairs, LANES, CHUNK), BF16),
            pltpu.VMEM((chunks, pairs, LANES, LANES), F32),
            pltpu.VMEM((pairs, LANES, LANES), F32),
            pltpu.VMEM((chunks, pairs, LANES, LANES), BF16),
            pltpu.VMEM((chunks, pairs, LANES, CHUNK), F32),
            pltpu.VMEM((2, 2 * WINDOW, WINDOW), F32),
            pltpu.VMEM((blocks, 2 * WINDOW, att_heads * WINDOW), F32),
            pltpu.VMEM((blocks, 2 * WINDOW, att_heads * WINDOW), BF16),
            pltpu.VMEM((blocks, 8, WINDOW), F32),
            pltpu.VMEM((packed, LANES), BF16),
            pltpu.VMEM((later, packed, LANES), BF16),
            pltpu.VMEM((rows, ret_w + att_w), BF16),
            pltpu.VMEM((others, out_rows, ret_w + att_w), BF16),
            pltpu.VMEM((2, n_tp * ret_w, model), BF16),
            pltpu.VMEM((out_rows, model), F32),
            pltpu.VMEM((pairs, LANES, LANES), F32),
            pltpu.VMEM((n_tp, 1, depth), F32),
            pltpu.VMEM((heads, 1, rows), F32),
            pltpu.VMEM((ret_w,), F32),
            pltpu.SMEM(sink.shape, F32),
            dma((4,)), dma((2,)), dma((n_tp, 6)), dma((2,)),
            dma((others, 2)), dma((others, 2)),
            dma((others, 2)), dma((others, 2)),
            dma((others, 2)), dma((others, 2)),
            dma((later,)), dma((later,)),
            dma, dma,
        ],
        compiler_params=pltpu.CompilerParams(
            collective_id=0, has_side_effects=True, vmem_limit_bytes=62 * 1024 * 1024
        ),
    )(
        tokens[0], in_gain.reshape(n_tp, 1, depth), rq, rk, rv, aq, ak, av,
        jnp.transpose(log_decay, (1, 0, 2)), ret_gain, sink, wr, wa,
    )
    return result[None]


def solution(mesh):
    n_sp, n_tp = mesh.shape["sp"], mesh.shape["tp"]
    return jax.shard_map(
        functools.partial(shards, n_sp, n_tp),
        mesh=mesh,
        in_specs=(
            P("fs", "sp", "tp"),
            P(),
            P(None, "tp"),
            P(None, "tp"),
            P(None, "tp"),
            P(None, "tp"),
            P(None, "tp"),
            P(None, "tp"),
            P("fs", "tp", "sp"),
            P("tp"),
            P("tp"),
            P("tp", None),
            P("tp", None),
        ),
        out_specs=P("fs", ("sp", "tp"), None),
        check_vma=False,
    )
```

```python
import functools

import jax
import jax.numpy as jnp
from jax import lax
from jax.experimental import pallas as pl
from jax.experimental.pallas import tpu as pltpu
from jax.sharding import PartitionSpec as P

HEAD_DIM = 64
WINDOW = 128
CHUNK = 128
LANES = 128
TILE = 256
EPS = 1e-06
F32 = jnp.float32
BF16 = jnp.bfloat16

NT = (((1,), (1,)), ((), ()))
TN = (((0,), (0,)), ((), ()))


def weave(*streams):
    order = []
    for k, stream in enumerate(streams):
        for i, piece in enumerate(stream):
            order.append(((i + 0.5) / len(stream), k, i, piece))
    for item in sorted(order, key=lambda entry: entry[:3]):
        item[3]()


def layer(
    n_sp, n_tp,
    tok, gain_in, rq, rk, rv, aq, ak, av, ld_in, rgain_in, sink_in, wr, wa,
    out,
    xb, wb, acc, pb, sq, inv, cr, eqr, ekr, dt, vt, ub, st, stb, ri, early, kd, va, sc, pw, dn, ao,
    rs, rw, msg, inbox, halo, sr, hb, hin, wo, oacc, gt,
    gain, ld, rgain, sink, small_sem, tok_sem, w_sem, wo_sem, x_send, x_recv, wo_send, wo_recv,
    h_send, h_recv, m_send, m_recv, s_send, s_recv, halo_send, halo_recv, ready,
):
    tp = lax.axis_index("tp")
    sp = lax.axis_index("sp")
    rows, depth = tok.shape
    ret_w, att_w, kv_w = rq.shape[1], aq.shape[1], ak.shape[1]
    heads = ld_in.shape[0]
    chunks = rows // CHUNK
    pairs = ret_w // LANES
    att_pairs = att_w // LANES
    att_heads = att_w // HEAD_DIM
    kv_heads = kv_w // HEAD_DIM
    group = att_heads // kv_heads
    out_rows = rows // n_tp
    model = depth * n_tp
    scale = HEAD_DIM ** (-0.5)
    half = rows // 2
    blocks = rows // WINDOW

    c_ak, c_av = 0, kv_w
    c_pairs = 2 * kv_w
    c_aq = c_pairs + 2 * ret_w
    c_rq = c_aq + att_w
    width = c_rq + ret_w
    parts = [(ak, 0, kv_w, c_ak), (av, 0, kv_w, c_av)]
    for p in range(pairs):
        parts.append((rk, p * LANES, LANES, c_pairs + p * 2 * LANES))
        parts.append((rv, p * LANES, LANES, c_pairs + p * 2 * LANES + LANES))
    parts += [(aq, 0, att_w, c_aq), (rq, 0, ret_w, c_rq)]
    pair_tiles = [
        slice(c_pairs + p * 2 * LANES, c_pairs + (p + 1) * 2 * LANES) for p in range(pairs)
    ]
    kv_tile = slice(c_ak, c_pairs)
    query_tiles = [slice(at, at + TILE) for at in range(c_aq, width, TILE)]

    def c_rk(p):
        return slice(c_pairs + p * 2 * LANES, c_pairs + p * 2 * LANES + LANES)

    def c_rv(p):
        return slice(c_pairs + p * 2 * LANES + LANES, c_pairs + (p + 1) * 2 * LANES)

    def load_tokens(i):
        span = pl.ds(i * half, half)
        return pltpu.make_async_copy(tok.at[span, :], xb.at[0, span, :], tok_sem.at[i])

    def load_weight(phase, i):
        owner = lax.rem(tp + phase, n_tp)
        ref, at, size, col = parts[i]
        return pltpu.make_async_copy(
            ref.at[pl.ds(owner * depth, depth), pl.ds(at, size)],
            wb.at[phase, :, pl.ds(col, size)],
            w_sem.at[phase + 1 if phase > 0 or i >= 4 else 0],
        )

    def wait_weights(group):
        cut = c_pairs + 2 * LANES
        ref = wb.at[max(group - 1, 0)]
        if group < 2:
            ref = ref.at[:, pl.ds(0, cut) if group == 0 else pl.ds(cut, width - cut)]
        pltpu.make_async_copy(ref, ref, w_sem.at[group]).wait()

    def load_exit(i):
        ref = (wr, wa)[i]
        return pltpu.make_async_copy(
            ref, wo.at[i, pl.ds(0, ref.shape[0]), :], wo_sem
        )

    def wait_exit():
        ref = wo.at[:, pl.ds(0, ret_w), :]
        pltpu.make_async_copy(ref, ref, wo_sem).wait()

    def all_tokens(q):
        return pltpu.make_async_remote_copy(
            src_ref=xb.at[0], dst_ref=xb.at[n_tp - q],
            send_sem=x_send.at[q - 1], recv_sem=x_recv.at[n_tp - q - 1],
            device_id={"tp": lax.rem(tp + q, n_tp)}, device_id_type=pl.DeviceIdType.MESH,
        )

    def all_exit(q):
        here_ = wo.at[:, pl.ds((n_tp - q) * ret_w, ret_w), :]
        return pltpu.make_async_remote_copy(
            src_ref=here_, dst_ref=here_,
            send_sem=wo_send.at[q - 1], recv_sem=wo_recv.at[n_tp - q - 1],
            device_id={"tp": lax.rem(tp + q, n_tp)}, device_id_type=pl.DeviceIdType.MESH,
        )

    def all_heads(q):
        target = lax.rem(tp + q, n_tp)
        return pltpu.make_async_remote_copy(
            src_ref=hb.at[pl.ds(target * out_rows, out_rows), :],
            dst_ref=hin.at[n_tp - q - 1],
            send_sem=h_send.at[q - 1], recv_sem=h_recv.at[n_tp - q - 1, 0],
            device_id={"tp": target}, device_id_type=pl.DeviceIdType.MESH,
        )

    def all_states(q):
        return pltpu.make_async_remote_copy(
            src_ref=msg, dst_ref=inbox.at[q - 1],
            send_sem=m_send.at[q - 1], recv_sem=m_recv.at[q - 1],
            device_id={"sp": lax.rem(sp + q, n_sp)}, device_id_type=pl.DeviceIdType.MESH,
        )

    def send_tokens(q, i):
        span = pl.ds(i * half, half)
        return pltpu.make_async_remote_copy(
            src_ref=xb.at[0, span, :], dst_ref=xb.at[n_tp - q, span, :],
            send_sem=x_send.at[q - 1], recv_sem=x_recv.at[n_tp - q - 1],
            device_id={"tp": lax.rem(tp + q, n_tp)}, device_id_type=pl.DeviceIdType.MESH,
        )

    def send_squares(q):
        return pltpu.make_async_remote_copy(
            src_ref=sr.at[0], dst_ref=sr.at[n_tp - q],
            send_sem=s_send.at[q - 1], recv_sem=s_recv.at[n_tp - q - 1],
            device_id={"tp": lax.rem(tp + q, n_tp)}, device_id_type=pl.DeviceIdType.MESH,
        )

    def send_exit(q, i):
        ref = (wr, wa)[i]
        return pltpu.make_async_remote_copy(
            src_ref=ref,
            dst_ref=wo.at[i, pl.ds((n_tp - q) * ref.shape[0], ref.shape[0]), :],
            send_sem=wo_send.at[q - 1], recv_sem=wo_recv.at[n_tp - q - 1],
            device_id={"tp": lax.rem(tp + q, n_tp)}, device_id_type=pl.DeviceIdType.MESH,
        )

    def send_heads(q, i):
        target = lax.rem(tp + q, n_tp)
        cols = pl.ds(i * ret_w, (ret_w, att_w)[i])
        return pltpu.make_async_remote_copy(
            src_ref=hb.at[pl.ds(target * out_rows, out_rows), cols],
            dst_ref=hin.at[n_tp - q - 1, :, cols],
            send_sem=h_send.at[q - 1], recv_sem=h_recv.at[n_tp - q - 1, i],
            device_id={"tp": target}, device_id_type=pl.DeviceIdType.MESH,
        )

    def send_state(q, p):
        span = pl.ds(0, 16 + HEAD_DIM) if p == 0 else pl.ds(16 + p * HEAD_DIM, HEAD_DIM)
        return pltpu.make_async_remote_copy(
            src_ref=msg.at[span, :], dst_ref=inbox.at[q - 1, span, :],
            send_sem=m_send.at[q - 1], recv_sem=m_recv.at[q - 1],
            device_id={"sp": lax.rem(sp + q, n_sp)}, device_id_type=pl.DeviceIdType.MESH,
        )

    def send_halo():
        cols = pl.ds(c_ak, 2 * kv_w)
        return pltpu.make_async_remote_copy(
            src_ref=pb.at[pl.ds(rows, WINDOW), cols],
            dst_ref=halo,
            send_sem=halo_send, recv_sem=halo_recv,
            device_id={"sp": lax.rem(sp + 1, n_sp)}, device_id_type=pl.DeviceIdType.MESH,
        )

    smalls = [
        pltpu.make_async_copy(src, dst, small_sem.at[i])
        for i, (src, dst) in enumerate(
            ((ld_in, ld), (gain_in, gain), (rgain_in, rgain), (sink_in, sink))
        )
    ]
    for copy in smalls:
        copy.start()
    barrier = pltpu.get_barrier_semaphore()
    for q in range(1, n_tp):
        pl.semaphore_signal(
            barrier, inc=1, device_id={"tp": lax.rem(tp + q, n_tp)},
            device_id_type=pl.DeviceIdType.MESH,
        )
    for q in range(1, n_sp):
        @pl.when(sp + q < n_sp)
        def _():
            pl.semaphore_signal(
                barrier, inc=1, device_id={"sp": lax.rem(sp + q, n_sp)},
                device_id_type=pl.DeviceIdType.MESH,
            )
    load_tokens(0).start()
    for i in range(4):
        load_weight(0, i).start()
    load_tokens(1).start()

    lane1 = lax.broadcasted_iota(jnp.int32, (1, LANES), 1)
    first_lanes = lane1 < HEAD_DIM
    half_masks = (
        jnp.where(first_lanes, scale, 0.0).astype(BF16),
        jnp.where(first_lanes, 0.0, scale).astype(BF16),
    )
    lane = lax.broadcasted_iota(jnp.int32, (CHUNK, LANES), 1)
    row = lax.broadcasted_iota(jnp.int32, (CHUNK, LANES), 0)
    same_head = (row < HEAD_DIM) == (lane < HEAD_DIM)
    before = row > lane
    early[...] = jnp.where(before, 1.0, 0.0).astype(BF16)

    pad = cr.shape[1]
    cr[...] = jnp.zeros_like(cr)
    for copy in smalls:
        copy.wait()
    for i in range(4, len(parts)):
        load_weight(0, i).start()
    for p in range(pairs):
        gt[p] = jnp.broadcast_to(
            rgain[p * LANES : (p + 1) * LANES].reshape(1, LANES), (LANES, LANES)
        ).T
    for h in range(heads):
        for c in range(chunks):
            cr[c, h : h + 1, :] = ld[h, :, c * CHUNK : (c + 1) * CHUNK]
    steps = cr[...].reshape(chunks * pad, CHUNK)
    top = steps.astype(BF16)
    rest = steps - top.astype(F32)
    mid = rest.astype(BF16)
    low = (rest - mid.astype(F32)).astype(BF16)
    upto = jnp.where(row <= lane, 1.0, 0.0).astype(BF16)
    sums = jnp.dot(
        jnp.concatenate([top, mid, low], axis=0), upto, preferred_element_type=F32
    )
    n_steps = chunks * pad
    cumulative = sums[:n_steps] + (sums[n_steps : 2 * n_steps] + sums[2 * n_steps :])
    cr[...] = cumulative.reshape(chunks, pad, CHUNK)
    eqr[...] = jnp.exp(cumulative).reshape(chunks, pad, CHUNK)
    ekr[...] = (jnp.exp(cumulative[:, CHUNK - 1 :] - cumulative) * scale).reshape(
        chunks, pad, CHUNK
    )
    filler = jnp.zeros((LANES - n_steps % LANES, CHUNK), F32)
    columns = jnp.concatenate([cumulative, filler], axis=0).T

    def decay(c, h):
        def piece():
            at = c * pad + h
            wide = jnp.broadcast_to(columns[:, at : at + 1], (CHUNK, LANES))
            gap = jnp.where(row <= lane, cr[c, h : h + 1, :] - wide, -jnp.inf)
            dt[c, h // 2, :, (h % 2) * CHUNK : (h % 2 + 1) * CHUNK] = jnp.exp(gap)

        return piece

    def scaled(i):
        def piece():
            span = slice(i * CHUNK, (i + 1) * CHUNK)
            x = xb[0, span, :].astype(F32)
            xb[0, span, :] = (x * gain[tp]).astype(BF16)
            squares = jnp.broadcast_to(
                jnp.sum(x * x, axis=1, keepdims=True), (CHUNK, LANES)
            )
            sq[span, :] = squares

        return piece

    def turn(i):
        def piece():
            sr[0, i : i + 1, :] = sq[i * CHUNK : (i + 1) * CHUNK, :].T[:1]

        return piece

    def invert(i):
        def piece():
            span = slice(i * CHUNK, (i + 1) * CHUNK)
            line = sr[1, i : i + 1, :]
            for phase in range(2, n_tp):
                line = line + sr[phase, i : i + 1, :]
            squares = sq[span, :] + jnp.broadcast_to(line, (LANES, CHUNK)).T
            inv[span, :] = lax.rsqrt(squares / model + EPS)

        return piece

    def project(phase, cols, i=0, parts_of=1):
        def piece():
            size = rows // parts_of
            span = slice(i * size, (i + 1) * size)
            total = jnp.dot(
                xb[phase, span, :], wb[phase, :, cols], preferred_element_type=F32
            )
            if phase > 0:
                total = acc[span, cols] + total
            if phase == n_tp - 1:
                wide = jnp.concatenate([inv[span, :]] * (TILE // LANES), axis=1)
                pb[WINDOW + i * size : WINDOW + (i + 1) * size, cols] = (
                    total * wide
                ).astype(BF16)
            else:
                acc[span, cols] = total

        return piece

    per_half = half // CHUNK
    last = n_tp - 1
    every = [kv_tile] + pair_tiles + query_tiles
    decays = [decay(c, h) for c in range(chunks) for h in range(heads)]
    weave(decays[:heads])
    decays = decays[heads:]
    load_tokens(0).wait()
    weave([scaled(i) for i in range(per_half)])
    pl.semaphore_wait(barrier, n_tp - 1 + sp)
    for q in range(1, n_tp):
        send_tokens(q, 0).start()
    for q in range(1, n_sp):
        @pl.when(sp >= q)
        def _():
            pl.semaphore_signal(
                ready, inc=1, device_id={"sp": lax.rem(sp + n_sp - q, n_sp)},
                device_id_type=pl.DeviceIdType.MESH,
            )
    load_tokens(1).wait()
    wait_weights(0)
    weave(
        [project(0, cols, 0, 2) for cols in every[:2]],
        [scaled(i) for i in range(per_half, chunks)],
    )
    for q in range(1, n_tp):
        send_tokens(q, 1).start()
    cut = len(decays) // len(every)
    weave(
        [project(0, cols, 1, 2) for cols in every[:2]],
        decays[:cut] + [turn(i) for i in range(chunks)],
    )
    for q in range(1, n_tp):
        send_squares(q).start()
    wait_weights(1)
    for phase in range(1, n_tp):
        for i in range(len(parts)):
            load_weight(phase, i).start()
    for q in range(1, n_tp):
        send_exit(q, 1).start()
    for i in range(1, -1, -1):
        load_exit(i).start()
    weave([project(0, cols) for cols in every[2:]], decays[cut:])
    for phase in range(1, n_tp):
        wait_weights(phase + 1)
        send_squares(n_tp - phase).wait_recv()
        all_tokens(n_tp - phase).wait_recv()
        if phase < last:
            weave([project(phase, cols) for cols in every])

    @pl.when(sp + 1 < n_sp)
    def _():
        pl.semaphore_wait(ready, n_sp - 1 - sp)


    def here(c):
        return pl.ds(pl.multiple_of(WINDOW + c * CHUNK, CHUNK), CHUNK)

    def own_state(p):
        def piece(c):
            turned = pb[here(c), c_rv(p)].T
            vt[c, p] = turned
            wide = turned.astype(F32)
            faded = jnp.concatenate(
                [
                    wide[:HEAD_DIM] * ekr[c, 2 * p : 2 * p + 1, :],
                    wide[HEAD_DIM:] * ekr[c, 2 * p + 1 : 2 * p + 2, :],
                ],
                axis=0,
            ).astype(BF16)
            added = jnp.dot(faded, pb[here(c), c_rk(p)], preferred_element_type=F32)
            ub[c, p] = jnp.where(same_head, added, 0.0)

        def pack():
            state = ub[0, p]
            for c in range(1, chunks):
                state = state * fade_row(c, p) + ub[c, p]
            msg[16 + p * HEAD_DIM : 16 + (p + 1) * HEAD_DIM, :] = (
                state[:HEAD_DIM] + state[HEAD_DIM:]
            ).astype(BF16)

        return [functools.partial(piece, c) for c in range(chunks)] + [pack]

    def fade_row(c, p):
        ends = [
            jnp.broadcast_to(eqr[c, h : h + 1, CHUNK - 1 :], (1, LANES))
            for h in (2 * p, 2 * p + 1)
        ]
        return jnp.where(first_lanes, ends[0], ends[1])

    totals = jnp.zeros((16, LANES), F32)
    row16 = lax.broadcasted_iota(jnp.int32, (16, LANES), 0)
    for p in range(pairs):
        total = fade_row(0, p)
        for c in range(1, chunks):
            total = total * fade_row(c, p)
        coarse = total.astype(BF16).astype(F32)
        totals = jnp.where(row16 == 2 * p, coarse, totals)
        totals = jnp.where(row16 == 2 * p + 1, total - coarse, totals)
    msg[:16, :] = totals.astype(BF16)

    def send_states(p):
        for q in range(n_sp - 1, 0, -1):
            @pl.when(sp + q < n_sp)
            def _():
                send_state(q, p).start()

    def double(i):
        def piece():
            span = slice(i * WINDOW, (i + 1) * WINDOW)
            for t in range(kv_w // LANES):
                keys = pb[span, c_ak + t * LANES : c_ak + (t + 1) * LANES]
                swapped = pltpu.roll(keys.astype(F32), HEAD_DIM, 1).astype(BF16)
                values = pb[span, c_av + t * LANES : c_av + (t + 1) * LANES].T
                for e in range(2):
                    g = 2 * t + e
                    kd[g, span, :] = jnp.where(first_lanes == (e == 0), keys, swapped)
                    va[i, g, :HEAD_DIM, :] = values[e * HEAD_DIM : (e + 1) * HEAD_DIM]
                    va[i, g, HEAD_DIM:, :] = jnp.ones((16, WINDOW), BF16)

        return piece

    def halves(cols):
        return [project(last, cols, i, 2) for i in range(2)]

    weave([invert(i) for i in range(chunks)])
    weave(halves(kv_tile) + halves(pair_tiles[0]))
    @pl.when(sp + 1 < n_sp)
    def _():
        send_halo().start()

    weave(own_state(0))
    send_states(0)
    weave(
        [piece for p in range(1, pairs) for piece in halves(pair_tiles[p])],
        [double(i) for i in range(1, blocks + 1)],
    )
    weave(*[own_state(p) for p in range(1, pairs)])
    for p in range(1, pairs):
        send_states(p)
    for q in range(1, n_tp):
        send_exit(q, 0).start()
    weave([piece for cols in query_tiles for piece in halves(cols)])

    per_part = blocks // n_tp

    def block(n):
        part = lax.rem(n // per_part + tp + 1, n_tp)
        return part * per_part + (n + 1) % per_part

    def band(n):
        return pl.ds(pl.multiple_of(block(n) * WINDOW, WINDOW), 2 * WINDOW)

    def score(n):
        def piece(g):
            queries = []
            for h in range(g * group, (g + 1) * group):
                at = c_aq + (h // 2) * LANES
                queries.append(pb[here(block(n)), at : at + LANES] * half_masks[h % 2])
            sc[n, :, g * group * WINDOW : (g + 1) * group * WINDOW] = lax.dot_general(
                kd[g, band(n), :], jnp.concatenate(queries, axis=0), NT,
                preferred_element_type=F32,
            )

        return [functools.partial(piece, g) for g in range(kv_heads)]

    def weigh(n):
        def piece(h):
            cols = slice(h * WINDOW, (h + 1) * WINDOW)
            outside = jnp.where((sp == 0) & (block(n) == 0), -jnp.inf, 0.0).astype(F32)
            s = jnp.where(before, sc[n, :WINDOW, cols] + outside, sc[n, WINDOW:, cols])
            sink_h = jnp.full((1, WINDOW), sink[h], F32)
            top = jnp.maximum(jnp.max(s, axis=0, keepdims=True), sink_h)
            dn[n, h : h + 1, :] = jnp.exp(sink_h - top)
            weights = jnp.exp(s - top).astype(BF16)
            older = weights * early[...]
            pw[n, :WINDOW, cols] = older
            pw[n, WINDOW:, cols] = weights - older

        return [functools.partial(piece, h) for h in range(att_heads)]

    def gather(n):
        def piece(g):
            left = jnp.concatenate([va[block(n), g], va[block(n) + 1, g]], axis=1)
            cols = slice(g * group * WINDOW, (g + 1) * group * WINDOW)
            total = jnp.dot(left, pw[n, :, cols], preferred_element_type=F32)
            for j in range(group):
                h = g * group + j
                cols = slice(j * WINDOW, (j + 1) * WINDOW)
                below = total[HEAD_DIM : HEAD_DIM + 1, cols] + dn[n, h : h + 1, :]
                ao[n, h * HEAD_DIM : (h + 1) * HEAD_DIM, :] = (
                    total[:HEAD_DIM, cols] * (1.0 / below)
                ).astype(BF16)

        def place():
            store = pl.ds(pl.multiple_of(block(n) * WINDOW, WINDOW), WINDOW)
            for p in range(att_pairs):
                hb[store, ret_w + p * LANES : ret_w + (p + 1) * LANES] = ao[
                    n, p * LANES : (p + 1) * LANES, :
                ].T

        return [functools.partial(piece, g) for g in range(kv_heads)] + [place]

    def relate(c):
        def piece(p):
            query = pb[here(c), c_rq + p * LANES : c_rq + (p + 1) * LANES]
            queries = jnp.concatenate([query * half_masks[e] for e in range(2)], axis=0)
            rs[c, p] = lax.dot_general(
                pb[here(c), c_rk(p)], queries, NT, preferred_element_type=F32
            )

        return [functools.partial(piece, p) for p in range(pairs)]

    def fade(c):
        def piece(p):
            rw[c, p] = (rs[c, p] * dt[c, p]).astype(BF16)

        return [functools.partial(piece, p) for p in range(pairs)]

    def recall(c):
        def piece(p):
            total = jnp.dot(vt[c, p], rw[c, p], preferred_element_type=F32)
            ri[c, p, :HEAD_DIM, :] = total[:HEAD_DIM, :CHUNK]
            ri[c, p, HEAD_DIM:, :] = total[HEAD_DIM:, CHUNK:]

        return [functools.partial(piece, p) for p in range(pairs)]

    for i in range(blocks + 2):
        if i % per_part == per_part - 1 and i < blocks:
            @pl.when((tp == n_tp - 1 - i // per_part) & (sp > 0))
            def _():
                send_halo().wait_recv()
                pb[:WINDOW, kv_tile] = halo[...]
                double(0)()

            @pl.when((tp == n_tp - 1 - i // per_part) & (sp == 0))
            def _():
                pb[:WINDOW, kv_tile] = jnp.zeros((WINDOW, 2 * kv_w), BF16)
                double(0)()

        first, second, third = (0 <= i - k < blocks for k in range(3))
        weave(
            (score(i) + relate(i) if first else [])
            + (gather(i - 2) + recall(i - 2) if third else []),
            weigh(i - 1) + fade(i - 1) if second else [],
        )
        for q in range(1, n_tp):
            if i - 1 == q * per_part:
                send_heads(q, 1).start()

    mine = pl.ds(pl.multiple_of(tp * out_rows, out_rows), out_rows)

    def leave(kind, n):
        def piece():
            cols = slice(n * TILE, (n + 1) * TILE)
            inner = slice(kind * ret_w, (kind + 1) * ret_w)
            left = jnp.concatenate(
                [hb[mine, inner]] + [hin[phase - 1, :, inner] for phase in range(1, n_tp)],
                axis=1,
            )
            total = jnp.dot(left, wo[kind, :, cols], preferred_element_type=F32)
            if kind == 1:
                oacc[:, cols] = total
            else:
                out[:, cols] = (oacc[:, cols] + total).astype(BF16)

        return piece

    st[...] = jnp.zeros_like(st)
    for q in range(n_sp - 1, 0, -1):
        @pl.when(sp >= q)
        def _():
            all_states(q).wait_recv()
            tail = inbox[q - 1, :16, :].astype(F32)
            for p in range(pairs):
                part = inbox[q - 1, 16 + p * HEAD_DIM : 16 + (p + 1) * HEAD_DIM, :].astype(F32)
                fade = tail[2 * p : 2 * p + 1] + tail[2 * p + 1 : 2 * p + 2]
                both = jnp.concatenate([part, part], axis=0)
                st[p] = st[p] * fade + jnp.where(same_head, both, 0.0)

    for p in range(pairs):
        state = st[p]
        for c in range(chunks):
            stb[c, p] = state.astype(BF16)
            if c + 1 < chunks:
                state = state * fade_row(c, p) + ub[c, p]

    def finish(c):
        def piece(p):
            query = pb[here(c), c_rq + p * LANES : c_rq + (p + 1) * LANES]
            carried = lax.dot_general(stb[c, p], query, NT, preferred_element_type=F32)
            normed = []
            for e in range(2):
                span = slice(e * HEAD_DIM, (e + 1) * HEAD_DIM)
                h = 2 * p + e
                r = ri[c, p, span, :] + carried[span] * eqr[c, h : h + 1, :]
                square = jnp.sum(r * r, axis=0, keepdims=True)
                normed.append(
                    (r * lax.rsqrt(square * (1.0 / HEAD_DIM) + EPS) * gt[p, span, :]).astype(BF16)
                )
            rows_c = pl.ds(pl.multiple_of(c * CHUNK, CHUNK), CHUNK)
            hb[rows_c, p * LANES : (p + 1) * LANES] = jnp.concatenate(normed, axis=0).T

        return [functools.partial(piece, p) for p in range(pairs)]

    each = chunks // n_tp
    for q in range(1, n_tp):
        first = lax.rem(tp + q, n_tp) * each
        weave([piece for i in range(each) for piece in finish(first + i)])
        send_heads(q, 0).start()
    wait_exit()
    for phase in range(1, n_tp):
        all_exit(n_tp - phase).wait_recv()
        send_heads(n_tp - phase, 1).wait_recv()
    weave(
        [leave(1, n) for n in range(model // TILE)],
        [piece for i in range(each) for piece in finish(tp * each + i)],
    )
    for phase in range(1, n_tp):
        send_heads(n_tp - phase, 0).wait_recv()
    weave([leave(0, n) for n in range(model // TILE)])
    for q in range(1, n_tp):
        send_squares(q).wait_send()
        all_tokens(q).wait_send()
        all_exit(q).wait_send()
        all_heads(q).wait_send()
    for q in range(1, n_sp):
        @pl.when(sp + q < n_sp)
        def _():
            all_states(q).wait_send()

    @pl.when(sp + 1 < n_sp)
    def _():
        send_halo().wait_send()


def shards(n_sp, n_tp, tokens, in_gain, rq, rk, rv, aq, ak, av, log_decay, ret_gain, sink, wr, wa):
    rows, depth = tokens.shape[1:]
    ret_w, att_w, kv_w = rq.shape[1], aq.shape[1], ak.shape[1]
    heads = log_decay.shape[1]
    model = depth * n_tp
    width = 3 * ret_w + att_w + 2 * kv_w
    chunks, pairs, blocks = rows // CHUNK, ret_w // LANES, rows // WINDOW
    att_heads = att_w // HEAD_DIM
    out_rows = rows // n_tp
    later = max(n_sp - 1, 1)
    others = max(n_tp - 1, 1)
    packed = pairs * HEAD_DIM + 16
    pad = 8
    hbm = pl.BlockSpec(memory_space=pltpu.HBM)
    dma = pltpu.SemaphoreType.DMA
    result = pl.pallas_call(
        functools.partial(layer, n_sp, n_tp),
        out_shape=pltpu.VMEM((out_rows, model), BF16),
        in_specs=[hbm] * 13,
        out_specs=pl.BlockSpec(memory_space=pltpu.VMEM),
        scratch_shapes=[
            pltpu.VMEM((n_tp, rows, depth), BF16),
            pltpu.VMEM((n_tp, depth, width), BF16),
            pltpu.VMEM((rows, width), F32),
            pltpu.VMEM((WINDOW + rows, width), BF16),
            pltpu.VMEM((rows, LANES), F32),
            pltpu.VMEM((rows, LANES), F32),
            pltpu.VMEM((chunks, pad, CHUNK), F32),
            pltpu.VMEM((chunks, pad, CHUNK), F32),
            pltpu.VMEM((chunks, pad, CHUNK), F32),
            pltpu.VMEM((chunks, pairs, CHUNK, 2 * CHUNK), F32),
            pltpu.VMEM((chunks, pairs, LANES, CHUNK), BF16),
            pltpu.VMEM((chunks, pairs, LANES, LANES), F32),
            pltpu.VMEM((pairs, LANES, LANES), F32),
            pltpu.VMEM((chunks, pairs, LANES, LANES), BF16),
            pltpu.VMEM((chunks, pairs, LANES, CHUNK), F32),
            pltpu.VMEM((WINDOW, WINDOW), BF16),
            pltpu.VMEM((kv_w // HEAD_DIM, WINDOW + rows, LANES), BF16),
            pltpu.VMEM((blocks + 1, kv_w // HEAD_DIM, HEAD_DIM + 16, WINDOW), BF16),
            pltpu.VMEM((blocks, 2 * WINDOW, att_heads * WINDOW), F32),
            pltpu.VMEM((blocks, 2 * WINDOW, att_heads * WINDOW), BF16),
            pltpu.VMEM((blocks, 8, WINDOW), F32),
            pltpu.VMEM((blocks, att_w, WINDOW), BF16),
            pltpu.VMEM((chunks, pairs, CHUNK, 2 * CHUNK), F32),
            pltpu.VMEM((chunks, pairs, CHUNK, 2 * CHUNK), BF16),
            pltpu.VMEM((packed, LANES), BF16),
            pltpu.VMEM((later, packed, LANES), BF16),
            pltpu.VMEM((WINDOW, 2 * kv_w), BF16),
            pltpu.VMEM((n_tp, 8, CHUNK), F32),
            pltpu.VMEM((rows, ret_w + att_w), BF16),
            pltpu.VMEM((others, out_rows, ret_w + att_w), BF16),
            pltpu.VMEM((2, n_tp * ret_w, model), BF16),
            pltpu.VMEM((out_rows, model), F32),
            pltpu.VMEM((pairs, LANES, LANES), F32),
            pltpu.VMEM((n_tp, 1, depth), F32),
            pltpu.VMEM((heads, 1, rows), F32),
            pltpu.VMEM((ret_w,), F32),
            pltpu.SMEM(sink.shape, F32),
            dma((4,)), dma((2,)), dma((n_tp + 1,)), dma,
            dma((others,)), dma((others,)),
            dma((others,)), dma((others,)),
            dma((others,)), dma((others, 2)),
            dma((later,)), dma((later,)),
            dma((others,)), dma((others,)),
            dma, dma, pltpu.SemaphoreType.REGULAR,
        ],
        compiler_params=pltpu.CompilerParams(
            collective_id=0, has_side_effects=True, vmem_limit_bytes=62 * 1024 * 1024
        ),
    )(
        tokens[0], in_gain.reshape(n_tp, 1, depth), rq, rk, rv, aq, ak, av,
        jnp.transpose(log_decay, (1, 0, 2)), ret_gain, sink, wr, wa,
    )
    return result[None]


def solution(mesh):
    n_sp, n_tp = mesh.shape["sp"], mesh.shape["tp"]
    return jax.shard_map(
        functools.partial(shards, n_sp, n_tp),
        mesh=mesh,
        in_specs=(
            P("fs", "sp", "tp"),
            P(),
            P(None, "tp"),
            P(None, "tp"),
            P(None, "tp"),
            P(None, "tp"),
            P(None, "tp"),
            P(None, "tp"),
            P("fs", "tp", "sp"),
            P("tp"),
            P("tp"),
            P("tp", None),
            P("tp", None),
        ),
        out_specs=P("fs", ("sp", "tp"), None),
        check_vma=False,
    )
```

```python
import functools

import jax
import jax.numpy as jnp
from jax import lax
from jax.experimental import pallas as pl
from jax.experimental.pallas import tpu as pltpu
from jax.sharding import PartitionSpec as P

HEAD_DIM = 64
WINDOW = 128
CHUNK = 128
LANES = 128
TILE = 256
EPS = 1e-06
F32 = jnp.float32
BF16 = jnp.bfloat16

NT = (((1,), (1,)), ((), ()))
TN = (((0,), (0,)), ((), ()))


def weave(*streams):
    order = []
    for k, stream in enumerate(streams):
        for i, piece in enumerate(stream):
            order.append(((i + 0.5) / len(stream), k, i, piece))
    for item in sorted(order, key=lambda entry: entry[:3]):
        item[3]()


def layer(
    n_sp, n_tp,
    tok, gain_in, rq, rk, rv, aq, ak, av, ld_in, rgain_in, sink_in, wr, wa,
    out,
    xb, wb, acc, pb, sq, inv, cr, eqr, ekr, dt, vt, ub, st, stb, ri, early, kd, va, sc, pw, dn, ao,
    rs, rw, msg, inbox, halo, sr, hb, hin, wo, oacc, gt,
    gain, ld, rgain, sink, small_sem, tok_sem, w_sem, wo_sem, x_send, x_recv, wo_send, wo_recv,
    h_send, h_recv, m_send, m_recv, s_send, s_recv, halo_send, halo_recv, ready,
):
    tp = lax.axis_index("tp")
    sp = lax.axis_index("sp")
    rows, depth = tok.shape
    ret_w, att_w, kv_w = rq.shape[1], aq.shape[1], ak.shape[1]
    heads = ld_in.shape[0]
    chunks = rows // CHUNK
    pairs = ret_w // LANES
    att_pairs = att_w // LANES
    att_heads = att_w // HEAD_DIM
    kv_heads = kv_w // HEAD_DIM
    group = att_heads // kv_heads
    out_rows = rows // n_tp
    model = depth * n_tp
    scale = HEAD_DIM ** (-0.5)
    half = rows // 2
    blocks = rows // WINDOW

    c_ak, c_av = 0, kv_w
    c_pairs = 2 * kv_w
    c_aq = c_pairs + 2 * ret_w
    c_rq = c_aq + att_w
    width = c_rq + ret_w
    parts = [(ak, 0, kv_w, c_ak), (av, 0, kv_w, c_av)]
    for p in range(pairs):
        parts.append((rk, p * LANES, LANES, c_pairs + p * 2 * LANES))
        parts.append((rv, p * LANES, LANES, c_pairs + p * 2 * LANES + LANES))
    parts += [(aq, 0, att_w, c_aq), (rq, 0, ret_w, c_rq)]
    pair_tiles = [
        slice(c_pairs + p * 2 * LANES, c_pairs + (p + 1) * 2 * LANES) for p in range(pairs)
    ]
    kv_tile = slice(c_ak, c_pairs)
    query_tiles = [slice(at, at + TILE) for at in range(c_aq, width, TILE)]

    def c_rk(p):
        return slice(c_pairs + p * 2 * LANES, c_pairs + p * 2 * LANES + LANES)

    def c_rv(p):
        return slice(c_pairs + p * 2 * LANES + LANES, c_pairs + (p + 1) * 2 * LANES)

    def load_tokens(i):
        span = pl.ds(i * half, half)
        return pltpu.make_async_copy(tok.at[span, :], xb.at[0, span, :], tok_sem.at[i])

    def load_weight(phase, i):
        owner = lax.rem(tp + phase, n_tp)
        ref, at, size, col = parts[i]
        return pltpu.make_async_copy(
            ref.at[pl.ds(owner * depth, depth), pl.ds(at, size)],
            wb.at[phase, :, pl.ds(col, size)],
            w_sem.at[phase + 1 if phase > 0 or i >= 4 else 0],
        )

    def wait_weights(group):
        cut = c_pairs + 2 * LANES
        ref = wb.at[max(group - 1, 0)]
        if group < 2:
            ref = ref.at[:, pl.ds(0, cut) if group == 0 else pl.ds(cut, width - cut)]
        pltpu.make_async_copy(ref, ref, w_sem.at[group]).wait()

    def load_exit(i):
        ref = (wr, wa)[i]
        return pltpu.make_async_copy(
            ref, wo.at[i, pl.ds(0, ref.shape[0]), :], wo_sem
        )

    def wait_exit():
        ref = wo.at[:, pl.ds(0, ret_w), :]
        pltpu.make_async_copy(ref, ref, wo_sem).wait()

    def all_tokens(q):
        return pltpu.make_async_remote_copy(
            src_ref=xb.at[0], dst_ref=xb.at[n_tp - q],
            send_sem=x_send.at[q - 1], recv_sem=x_recv.at[n_tp - q - 1],
            device_id={"tp": lax.rem(tp + q, n_tp)}, device_id_type=pl.DeviceIdType.MESH,
        )

    def all_exit(q):
        here_ = wo.at[:, pl.ds((n_tp - q) * ret_w, ret_w), :]
        return pltpu.make_async_remote_copy(
            src_ref=here_, dst_ref=here_,
            send_sem=wo_send.at[q - 1], recv_sem=wo_recv.at[n_tp - q - 1, 0],
            device_id={"tp": lax.rem(tp + q, n_tp)}, device_id_type=pl.DeviceIdType.MESH,
        )

    def all_heads(q):
        target = lax.rem(tp + q, n_tp)
        return pltpu.make_async_remote_copy(
            src_ref=hb.at[pl.ds(target * out_rows, out_rows), :],
            dst_ref=hin.at[n_tp - q - 1],
            send_sem=h_send.at[q - 1], recv_sem=h_recv.at[n_tp - q - 1, 0],
            device_id={"tp": target}, device_id_type=pl.DeviceIdType.MESH,
        )

    def all_states(q):
        return pltpu.make_async_remote_copy(
            src_ref=msg, dst_ref=inbox.at[q - 1],
            send_sem=m_send.at[q - 1], recv_sem=m_recv.at[q - 1],
            device_id={"sp": lax.rem(sp + q, n_sp)}, device_id_type=pl.DeviceIdType.MESH,
        )

    def send_tokens(q, i):
        span = pl.ds(i * half, half)
        return pltpu.make_async_remote_copy(
            src_ref=xb.at[0, span, :], dst_ref=xb.at[n_tp - q, span, :],
            send_sem=x_send.at[q - 1], recv_sem=x_recv.at[n_tp - q - 1],
            device_id={"tp": lax.rem(tp + q, n_tp)}, device_id_type=pl.DeviceIdType.MESH,
        )

    def send_squares(q):
        return pltpu.make_async_remote_copy(
            src_ref=sr.at[0], dst_ref=sr.at[n_tp - q],
            send_sem=s_send.at[q - 1], recv_sem=s_recv.at[n_tp - q - 1],
            device_id={"tp": lax.rem(tp + q, n_tp)}, device_id_type=pl.DeviceIdType.MESH,
        )

    def send_exit(q, i):
        ref = (wr, wa)[i]
        return pltpu.make_async_remote_copy(
            src_ref=wo.at[i, pl.ds(0, ref.shape[0]), :],
            dst_ref=wo.at[i, pl.ds((n_tp - q) * ref.shape[0], ref.shape[0]), :],
            send_sem=wo_send.at[q - 1], recv_sem=wo_recv.at[n_tp - q - 1, i],
            device_id={"tp": lax.rem(tp + q, n_tp)}, device_id_type=pl.DeviceIdType.MESH,
        )

    def send_heads(q, i):
        target = lax.rem(tp + q, n_tp)
        cols = pl.ds(i * ret_w, (ret_w, att_w)[i])
        return pltpu.make_async_remote_copy(
            src_ref=hb.at[pl.ds(target * out_rows, out_rows), cols],
            dst_ref=hin.at[n_tp - q - 1, :, cols],
            send_sem=h_send.at[q - 1], recv_sem=h_recv.at[n_tp - q - 1, i],
            device_id={"tp": target}, device_id_type=pl.DeviceIdType.MESH,
        )

    def send_state(q, p):
        span = pl.ds(0, 16 + HEAD_DIM) if p == 0 else pl.ds(16 + p * HEAD_DIM, HEAD_DIM)
        return pltpu.make_async_remote_copy(
            src_ref=msg.at[span, :], dst_ref=inbox.at[q - 1, span, :],
            send_sem=m_send.at[q - 1], recv_sem=m_recv.at[q - 1],
            device_id={"sp": lax.rem(sp + q, n_sp)}, device_id_type=pl.DeviceIdType.MESH,
        )

    def send_halo():
        cols = pl.ds(c_ak, 2 * kv_w)
        return pltpu.make_async_remote_copy(
            src_ref=pb.at[pl.ds(rows, WINDOW), cols],
            dst_ref=halo,
            send_sem=halo_send, recv_sem=halo_recv,
            device_id={"sp": lax.rem(sp + 1, n_sp)}, device_id_type=pl.DeviceIdType.MESH,
        )

    smalls = [
        pltpu.make_async_copy(src, dst, small_sem.at[i])
        for i, (src, dst) in enumerate(
            ((ld_in, ld), (gain_in, gain), (rgain_in, rgain), (sink_in, sink))
        )
    ]
    for copy in smalls:
        copy.start()
    barrier = pltpu.get_barrier_semaphore()
    for q in range(1, n_tp):
        pl.semaphore_signal(
            barrier, inc=1, device_id={"tp": lax.rem(tp + q, n_tp)},
            device_id_type=pl.DeviceIdType.MESH,
        )
    for q in range(1, n_sp):
        @pl.when(sp + q < n_sp)
        def _():
            pl.semaphore_signal(
                barrier, inc=1, device_id={"sp": lax.rem(sp + q, n_sp)},
                device_id_type=pl.DeviceIdType.MESH,
            )
    load_tokens(0).start()
    for i in range(4):
        load_weight(0, i).start()
    load_tokens(1).start()

    lane1 = lax.broadcasted_iota(jnp.int32, (1, LANES), 1)
    first_lanes = lane1 < HEAD_DIM
    half_masks = (
        jnp.where(first_lanes, scale, 0.0).astype(BF16),
        jnp.where(first_lanes, 0.0, scale).astype(BF16),
    )
    lane = lax.broadcasted_iota(jnp.int32, (CHUNK, LANES), 1)
    row = lax.broadcasted_iota(jnp.int32, (CHUNK, LANES), 0)
    same_head = (row < HEAD_DIM) == (lane < HEAD_DIM)
    before = row > lane
    early[...] = jnp.where(before, 1.0, 0.0).astype(BF16)

    pad = cr.shape[1]
    cr[...] = jnp.zeros_like(cr)
    for copy in smalls:
        copy.wait()
    for i in range(4, len(parts)):
        load_weight(0, i).start()
    for p in range(pairs):
        gt[p] = jnp.broadcast_to(
            rgain[p * LANES : (p + 1) * LANES].reshape(1, LANES), (LANES, LANES)
        ).T
    for h in range(heads):
        for c in range(chunks):
            cr[c, h : h + 1, :] = ld[h, :, c * CHUNK : (c + 1) * CHUNK]
    steps = cr[...].reshape(chunks * pad, CHUNK)
    top = steps.astype(BF16)
    rest = steps - top.astype(F32)
    mid = rest.astype(BF16)
    low = (rest - mid.astype(F32)).astype(BF16)
    upto = jnp.where(row <= lane, 1.0, 0.0).astype(BF16)
    sums = jnp.dot(
        jnp.concatenate([top, mid, low], axis=0), upto, preferred_element_type=F32
    )
    n_steps = chunks * pad
    cumulative = sums[:n_steps] + (sums[n_steps : 2 * n_steps] + sums[2 * n_steps :])
    cr[...] = cumulative.reshape(chunks, pad, CHUNK)
    eqr[...] = jnp.exp(cumulative).reshape(chunks, pad, CHUNK)
    ekr[...] = (jnp.exp(cumulative[:, CHUNK - 1 :] - cumulative) * scale).reshape(
        chunks, pad, CHUNK
    )
    filler = jnp.zeros((LANES - n_steps % LANES, CHUNK), F32)
    columns = jnp.concatenate([cumulative, filler], axis=0).T

    def decay(c, h):
        def piece():
            at = c * pad + h
            wide = jnp.broadcast_to(columns[:, at : at + 1], (CHUNK, LANES))
            gap = jnp.where(row <= lane, cr[c, h : h + 1, :] - wide, -jnp.inf)
            dt[c, h // 2, :, (h % 2) * CHUNK : (h % 2 + 1) * CHUNK] = jnp.exp(gap)

        return piece

    def scaled(i):
        def piece():
            span = slice(i * CHUNK, (i + 1) * CHUNK)
            x = xb[0, span, :].astype(F32)
            xb[0, span, :] = (x * gain[tp]).astype(BF16)
            squares = jnp.broadcast_to(
                jnp.sum(x * x, axis=1, keepdims=True), (CHUNK, LANES)
            )
            sq[span, :] = squares

        return piece

    def turn(i):
        def piece():
            sr[0, i : i + 1, :] = sq[i * CHUNK : (i + 1) * CHUNK, :].T[:1]

        return piece

    def invert(i):
        def piece():
            span = slice(i * CHUNK, (i + 1) * CHUNK)
            line = sr[1, i : i + 1, :]
            for phase in range(2, n_tp):
                line = line + sr[phase, i : i + 1, :]
            squares = sq[span, :] + jnp.broadcast_to(line, (LANES, CHUNK)).T
            inv[span, :] = lax.rsqrt(squares / model + EPS)

        return piece

    def project(phase, cols, i=0, parts_of=1):
        def piece():
            size = rows // parts_of
            span = slice(i * size, (i + 1) * size)
            total = jnp.dot(
                xb[phase, span, :], wb[phase, :, cols], preferred_element_type=F32
            )
            if phase > 0:
                total = acc[span, cols] + total
            if phase == n_tp - 1:
                wide = jnp.concatenate([inv[span, :]] * (TILE // LANES), axis=1)
                pb[WINDOW + i * size : WINDOW + (i + 1) * size, cols] = (
                    total * wide
                ).astype(BF16)
            else:
                acc[span, cols] = total

        return piece

    per_half = half // CHUNK
    last = n_tp - 1
    every = [kv_tile] + pair_tiles + query_tiles
    decays = [decay(c, h) for c in range(chunks) for h in range(heads)]
    weave(decays[:heads])
    decays = decays[heads:]
    load_tokens(0).wait()
    weave([scaled(i) for i in range(per_half)])
    pl.semaphore_wait(barrier, n_tp - 1 + sp)
    for q in range(1, n_tp):
        send_tokens(q, 0).start()
    for q in range(1, n_sp):
        @pl.when(sp >= q)
        def _():
            pl.semaphore_signal(
                ready, inc=1, device_id={"sp": lax.rem(sp + n_sp - q, n_sp)},
                device_id_type=pl.DeviceIdType.MESH,
            )
    load_tokens(1).wait()
    wait_weights(0)
    weave(
        [project(0, cols, 0, 2) for cols in every[:2]],
        [scaled(i) for i in range(per_half, chunks)],
    )
    for q in range(1, n_tp):
        send_tokens(q, 1).start()
    cut = len(decays) // len(every)
    weave(
        [project(0, cols, 1, 2) for cols in every[:2]],
        decays[:cut] + [turn(i) for i in range(chunks)],
    )
    for q in range(1, n_tp):
        send_squares(q).start()
    wait_weights(1)
    for phase in range(1, n_tp):
        for i in range(len(parts)):
            load_weight(phase, i).start()
    for i in range(1, -1, -1):
        load_exit(i).start()
    weave([project(0, cols, i, 2) for cols in every[2:] for i in range(2)], decays[cut:])
    for phase in range(1, n_tp):
        wait_weights(phase + 1)
        send_squares(n_tp - phase).wait_recv()
        all_tokens(n_tp - phase).wait_recv()
        if phase < last:
            weave([project(phase, cols) for cols in every])

    def here(c):
        return pl.ds(pl.multiple_of(WINDOW + c * CHUNK, CHUNK), CHUNK)

    def own_state(p):
        def piece(c):
            turned = pb[here(c), c_rv(p)].T
            vt[c, p] = turned
            wide = turned.astype(F32)
            faded = jnp.concatenate(
                [
                    wide[:HEAD_DIM] * ekr[c, 2 * p : 2 * p + 1, :],
                    wide[HEAD_DIM:] * ekr[c, 2 * p + 1 : 2 * p + 2, :],
                ],
                axis=0,
            ).astype(BF16)
            added = jnp.dot(faded, pb[here(c), c_rk(p)], preferred_element_type=F32)
            ub[c, p] = jnp.where(same_head, added, 0.0)

        def pack():
            state = ub[0, p]
            for c in range(1, chunks):
                state = state * fade_row(c, p) + ub[c, p]
            msg[16 + p * HEAD_DIM : 16 + (p + 1) * HEAD_DIM, :] = (
                state[:HEAD_DIM] + state[HEAD_DIM:]
            ).astype(BF16)

        return [functools.partial(piece, c) for c in range(chunks)] + [pack]

    def fade_row(c, p):
        ends = [
            jnp.broadcast_to(eqr[c, h : h + 1, CHUNK - 1 :], (1, LANES))
            for h in (2 * p, 2 * p + 1)
        ]
        return jnp.where(first_lanes, ends[0], ends[1])

    totals = jnp.zeros((16, LANES), F32)
    row16 = lax.broadcasted_iota(jnp.int32, (16, LANES), 0)
    for p in range(pairs):
        total = fade_row(0, p)
        for c in range(1, chunks):
            total = total * fade_row(c, p)
        coarse = total.astype(BF16).astype(F32)
        totals = jnp.where(row16 == 2 * p, coarse, totals)
        totals = jnp.where(row16 == 2 * p + 1, total - coarse, totals)
    msg[:16, :] = totals.astype(BF16)

    def send_states(p):
        for q in range(n_sp - 1, 0, -1):
            @pl.when(sp + q < n_sp)
            def _():
                send_state(q, p).start()

    def double(i):
        def piece():
            span = slice(i * WINDOW, (i + 1) * WINDOW)
            for t in range(kv_w // LANES):
                keys = pb[span, c_ak + t * LANES : c_ak + (t + 1) * LANES]
                swapped = pltpu.roll(keys.astype(F32), HEAD_DIM, 1).astype(BF16)
                values = pb[span, c_av + t * LANES : c_av + (t + 1) * LANES].T
                for e in range(2):
                    g = 2 * t + e
                    kd[g, span, :] = jnp.where(first_lanes == (e == 0), keys, swapped)
                    va[i, g, :HEAD_DIM, :] = values[e * HEAD_DIM : (e + 1) * HEAD_DIM]
                    va[i, g, HEAD_DIM:, :] = jnp.ones((16, WINDOW), BF16)

        return piece

    def halves(cols):
        return [project(last, cols, i, 2) for i in range(2)]

    weave([invert(i) for i in range(chunks)])
    weave(halves(kv_tile) + halves(pair_tiles[0]))
    @pl.when(sp + 1 < n_sp)
    def _():
        pl.semaphore_wait(ready, n_sp - 1 - sp)
        send_halo().start()

    weave(own_state(0))
    send_states(0)
    weave(
        [piece for p in range(1, pairs) for piece in halves(pair_tiles[p])],
        [double(i) for i in range(1, blocks + 1)],
    )
    weave(*[own_state(p) for p in range(1, pairs)])
    for p in range(1, pairs):
        send_states(p)
    wait_exit()
    for q in range(1, n_tp):
        send_exit(q, 1).start()
    weave([piece for cols in query_tiles for piece in halves(cols)])

    per_part = blocks // n_tp

    def block(n):
        part = lax.rem(n // per_part + tp + 1, n_tp)
        return part * per_part + (n + 1) % per_part

    def band(n):
        return pl.ds(pl.multiple_of(block(n) * WINDOW, WINDOW), 2 * WINDOW)

    def score(n):
        def piece(g):
            queries = []
            for h in range(g * group, (g + 1) * group):
                at = c_aq + (h // 2) * LANES
                queries.append(pb[here(block(n)), at : at + LANES] * half_masks[h % 2])
            sc[n, :, g * group * WINDOW : (g + 1) * group * WINDOW] = lax.dot_general(
                kd[g, band(n), :], jnp.concatenate(queries, axis=0), NT,
                preferred_element_type=F32,
            )

        return [functools.partial(piece, g) for g in range(kv_heads)]

    def weigh(n):
        def piece(h):
            cols = slice(h * WINDOW, (h + 1) * WINDOW)
            outside = jnp.where((sp == 0) & (block(n) == 0), -jnp.inf, 0.0).astype(F32)
            s = jnp.where(before, sc[n, :WINDOW, cols] + outside, sc[n, WINDOW:, cols])
            sink_h = jnp.full((1, WINDOW), sink[h], F32)
            top = jnp.maximum(jnp.max(s, axis=0, keepdims=True), sink_h)
            dn[n, h : h + 1, :] = jnp.exp(sink_h - top)
            weights = jnp.exp(s - top).astype(BF16)
            older = weights * early[...]
            pw[n, :WINDOW, cols] = older
            pw[n, WINDOW:, cols] = weights - older

        return [functools.partial(piece, h) for h in range(att_heads)]

    def gather(n):
        def piece(g):
            left = jnp.concatenate([va[block(n), g], va[block(n) + 1, g]], axis=1)
            cols = slice(g * group * WINDOW, (g + 1) * group * WINDOW)
            total = jnp.dot(left, pw[n, :, cols], preferred_element_type=F32)
            for j in range(group):
                h = g * group + j
                cols = slice(j * WINDOW, (j + 1) * WINDOW)
                below = total[HEAD_DIM : HEAD_DIM + 1, cols] + dn[n, h : h + 1, :]
                ao[n, h * HEAD_DIM : (h + 1) * HEAD_DIM, :] = (
                    total[:HEAD_DIM, cols] * (1.0 / below)
                ).astype(BF16)

        def place():
            store = pl.ds(pl.multiple_of(block(n) * WINDOW, WINDOW), WINDOW)
            for p in range(att_pairs):
                hb[store, ret_w + p * LANES : ret_w + (p + 1) * LANES] = ao[
                    n, p * LANES : (p + 1) * LANES, :
                ].T

        return [functools.partial(piece, g) for g in range(kv_heads)] + [place]

    def relate(c):
        def piece(p):
            query = pb[here(c), c_rq + p * LANES : c_rq + (p + 1) * LANES]
            queries = jnp.concatenate([query * half_masks[e] for e in range(2)], axis=0)
            rs[c, p] = lax.dot_general(
                pb[here(c), c_rk(p)], queries, NT, preferred_element_type=F32
            )

        return [functools.partial(piece, p) for p in range(pairs)]

    def fade(c):
        def piece(p):
            rw[c, p] = (rs[c, p] * dt[c, p]).astype(BF16)

        return [functools.partial(piece, p) for p in range(pairs)]

    def recall(c):
        def piece(p):
            total = jnp.dot(vt[c, p], rw[c, p], preferred_element_type=F32)
            ri[c, p, :HEAD_DIM, :] = total[:HEAD_DIM, :CHUNK]
            ri[c, p, HEAD_DIM:, :] = total[HEAD_DIM:, CHUNK:]

        return [functools.partial(piece, p) for p in range(pairs)]

    for i in range(blocks + 2):
        if i % per_part == per_part - 1 and i < blocks:
            @pl.when((tp == n_tp - 1 - i // per_part) & (sp > 0))
            def _():
                send_halo().wait_recv()
                pb[:WINDOW, kv_tile] = halo[...]
                double(0)()

            @pl.when((tp == n_tp - 1 - i // per_part) & (sp == 0))
            def _():
                pb[:WINDOW, kv_tile] = jnp.zeros((WINDOW, 2 * kv_w), BF16)
                double(0)()

        first, second, third = (0 <= i - k < blocks for k in range(3))
        weave(
            (score(i) + relate(i) if first else [])
            + (gather(i - 2) + recall(i - 2) if third else []),
            weigh(i - 1) + fade(i - 1) if second else [],
        )
        for q in range(1, n_tp):
            if i - 1 == q * per_part:
                send_heads(q, 1).start()
                send_exit(q, 0).start()

    mine = pl.ds(pl.multiple_of(tp * out_rows, out_rows), out_rows)

    def leave(kind, n):
        def piece():
            cols = slice(n * TILE, (n + 1) * TILE)
            inner = slice(kind * ret_w, (kind + 1) * ret_w)
            left = jnp.concatenate(
                [hb[mine, inner]] + [hin[phase - 1, :, inner] for phase in range(1, n_tp)],
                axis=1,
            )
            total = jnp.dot(left, wo[kind, :, cols], preferred_element_type=F32)
            if kind == 1:
                oacc[:, cols] = total
            else:
                out[:, cols] = (oacc[:, cols] + total).astype(BF16)

        return piece

    for phase in range(1, n_tp):
        send_exit(n_tp - phase, 1).wait_recv()
        send_heads(n_tp - phase, 1).wait_recv()
    exits = [leave(1, n) for n in range(model // TILE)]
    share = len(exits) // 2
    weave(exits[:share])
    st[...] = jnp.zeros_like(st)
    for q in range(n_sp - 1, 0, -1):
        @pl.when(sp >= q)
        def _():
            all_states(q).wait_recv()
            tail = inbox[q - 1, :16, :].astype(F32)
            for p in range(pairs):
                part = inbox[q - 1, 16 + p * HEAD_DIM : 16 + (p + 1) * HEAD_DIM, :].astype(F32)
                fade = tail[2 * p : 2 * p + 1] + tail[2 * p + 1 : 2 * p + 2]
                both = jnp.concatenate([part, part], axis=0)
                st[p] = st[p] * fade + jnp.where(same_head, both, 0.0)

    for p in range(pairs):
        state = st[p]
        for c in range(chunks):
            stb[c, p] = state.astype(BF16)
            if c + 1 < chunks:
                state = state * fade_row(c, p) + ub[c, p]

    def finish(c):
        def piece(p):
            query = pb[here(c), c_rq + p * LANES : c_rq + (p + 1) * LANES]
            carried = lax.dot_general(stb[c, p], query, NT, preferred_element_type=F32)
            normed = []
            for e in range(2):
                span = slice(e * HEAD_DIM, (e + 1) * HEAD_DIM)
                h = 2 * p + e
                r = ri[c, p, span, :] + carried[span] * eqr[c, h : h + 1, :]
                square = jnp.sum(r * r, axis=0, keepdims=True)
                normed.append(
                    (r * lax.rsqrt(square * (1.0 / HEAD_DIM) + EPS) * gt[p, span, :]).astype(BF16)
                )
            rows_c = pl.ds(pl.multiple_of(c * CHUNK, CHUNK), CHUNK)
            hb[rows_c, p * LANES : (p + 1) * LANES] = jnp.concatenate(normed, axis=0).T

        return [functools.partial(piece, p) for p in range(pairs)]

    each = chunks // n_tp
    for q in range(1, n_tp):
        first = lax.rem(tp + q, n_tp) * each
        weave([piece for i in range(each) for piece in finish(first + i)])
        send_heads(q, 0).start()
    weave(
        [leave(1, n) for n in range(model // TILE)],
        [piece for i in range(each) for piece in finish(tp * each + i)],
    )
    for phase in range(1, n_tp):
        send_exit(n_tp - phase, 0).wait_recv()
        send_heads(n_tp - phase, 0).wait_recv()
    weave([leave(0, n) for n in range(model // TILE)])
    for q in range(1, n_tp):
        send_squares(q).wait_send()
        all_tokens(q).wait_send()
        all_exit(q).wait_send()
        all_heads(q).wait_send()
    for q in range(1, n_sp):
        @pl.when(sp + q < n_sp)
        def _():
            all_states(q).wait_send()

    @pl.when(sp + 1 < n_sp)
    def _():
        send_halo().wait_send()


def shards(n_sp, n_tp, tokens, in_gain, rq, rk, rv, aq, ak, av, log_decay, ret_gain, sink, wr, wa):
    rows, depth = tokens.shape[1:]
    ret_w, att_w, kv_w = rq.shape[1], aq.shape[1], ak.shape[1]
    heads = log_decay.shape[1]
    model = depth * n_tp
    width = 3 * ret_w + att_w + 2 * kv_w
    chunks, pairs, blocks = rows // CHUNK, ret_w // LANES, rows // WINDOW
    att_heads = att_w // HEAD_DIM
    out_rows = rows // n_tp
    later = max(n_sp - 1, 1)
    others = max(n_tp - 1, 1)
    packed = pairs * HEAD_DIM + 16
    pad = 8
    hbm = pl.BlockSpec(memory_space=pltpu.HBM)
    dma = pltpu.SemaphoreType.DMA
    result = pl.pallas_call(
        functools.partial(layer, n_sp, n_tp),
        out_shape=pltpu.VMEM((out_rows, model), BF16),
        in_specs=[hbm] * 13,
        out_specs=pl.BlockSpec(memory_space=pltpu.VMEM),
        scratch_shapes=[
            pltpu.VMEM((n_tp, rows, depth), BF16),
            pltpu.VMEM((n_tp, depth, width), BF16),
            pltpu.VMEM((rows, width), F32),
            pltpu.VMEM((WINDOW + rows, width), BF16),
            pltpu.VMEM((rows, LANES), F32),
            pltpu.VMEM((rows, LANES), F32),
            pltpu.VMEM((chunks, pad, CHUNK), F32),
            pltpu.VMEM((chunks, pad, CHUNK), F32),
            pltpu.VMEM((chunks, pad, CHUNK), F32),
            pltpu.VMEM((chunks, pairs, CHUNK, 2 * CHUNK), F32),
            pltpu.VMEM((chunks, pairs, LANES, CHUNK), BF16),
            pltpu.VMEM((chunks, pairs, LANES, LANES), F32),
            pltpu.VMEM((pairs, LANES, LANES), F32),
            pltpu.VMEM((chunks, pairs, LANES, LANES), BF16),
            pltpu.VMEM((chunks, pairs, LANES, CHUNK), F32),
            pltpu.VMEM((WINDOW, WINDOW), BF16),
            pltpu.VMEM((kv_w // HEAD_DIM, WINDOW + rows, LANES), BF16),
            pltpu.VMEM((blocks + 1, kv_w // HEAD_DIM, HEAD_DIM + 16, WINDOW), BF16),
            pltpu.VMEM((blocks, 2 * WINDOW, att_heads * WINDOW), F32),
            pltpu.VMEM((blocks, 2 * WINDOW, att_heads * WINDOW), BF16),
            pltpu.VMEM((blocks, 8, WINDOW), F32),
            pltpu.VMEM((blocks, att_w, WINDOW), BF16),
            pltpu.VMEM((chunks, pairs, CHUNK, 2 * CHUNK), F32),
            pltpu.VMEM((chunks, pairs, CHUNK, 2 * CHUNK), BF16),
            pltpu.VMEM((packed, LANES), BF16),
            pltpu.VMEM((later, packed, LANES), BF16),
            pltpu.VMEM((WINDOW, 2 * kv_w), BF16),
            pltpu.VMEM((n_tp, 8, CHUNK), F32),
            pltpu.VMEM((rows, ret_w + att_w), BF16),
            pltpu.VMEM((others, out_rows, ret_w + att_w), BF16),
            pltpu.VMEM((2, n_tp * ret_w, model), BF16),
            pltpu.VMEM((out_rows, model), F32),
            pltpu.VMEM((pairs, LANES, LANES), F32),
            pltpu.VMEM((n_tp, 1, depth), F32),
            pltpu.VMEM((heads, 1, rows), F32),
            pltpu.VMEM((ret_w,), F32),
            pltpu.SMEM(sink.shape, F32),
            dma((4,)), dma((2,)), dma((n_tp + 1,)), dma,
            dma((others,)), dma((others,)),
            dma((others,)), dma((others, 2)),
            dma((others,)), dma((others, 2)),
            dma((later,)), dma((later,)),
            dma((others,)), dma((others,)),
            dma, dma, pltpu.SemaphoreType.REGULAR,
        ],
        compiler_params=pltpu.CompilerParams(
            collective_id=0, has_side_effects=True, vmem_limit_bytes=62 * 1024 * 1024
        ),
    )(
        tokens[0], in_gain.reshape(n_tp, 1, depth), rq, rk, rv, aq, ak, av,
        jnp.transpose(log_decay, (1, 0, 2)), ret_gain, sink, wr, wa,
    )
    return result[None]


def solution(mesh):
    n_sp, n_tp = mesh.shape["sp"], mesh.shape["tp"]
    return jax.shard_map(
        functools.partial(shards, n_sp, n_tp),
        mesh=mesh,
        in_specs=(
            P("fs", "sp", "tp"),
            P(),
            P(None, "tp"),
            P(None, "tp"),
            P(None, "tp"),
            P(None, "tp"),
            P(None, "tp"),
            P(None, "tp"),
            P("fs", "tp", "sp"),
            P("tp"),
            P("tp"),
            P("tp", None),
            P("tp", None),
        ),
        out_specs=P("fs", ("sp", "tp"), None),
        check_vma=False,
    )
```

```python
import functools

import jax
import jax.numpy as jnp
from jax import lax
from jax.experimental import pallas as pl
from jax.experimental.pallas import tpu as pltpu
from jax.sharding import PartitionSpec as P

HEAD_DIM = 64
WINDOW = 128
CHUNK = 128
LANES = 128
TILE = 256
PARTS = 4
EPS = 1e-06
F32 = jnp.float32
BF16 = jnp.bfloat16

NT = (((1,), (1,)), ((), ()))
TN = (((0,), (0,)), ((), ()))


def weave(*streams):
    order = []
    for k, stream in enumerate(streams):
        for i, piece in enumerate(stream):
            order.append(((i + 0.5) / len(stream), k, i, piece))
    for item in sorted(order, key=lambda entry: entry[:3]):
        item[3]()


def layer(
    n_sp, n_tp,
    tok, gain_in, rq, rk, rv, aq, ak, av, ld_in, rgain_in, sink_in, wr, wa,
    out,
    xb, wb, acc, pb, sq, inv, cr, eqr, ekr, dt, vt, ub, st, stb, ri, early, kd, va, sc, pw, dn, ao,
    rs, rw, msg, inbox, tot, tin, halo, sr, hb, hin, wo, oacc, gt,
    gain, ld, rgain, sink, small_sem, tok_sem, w_sem, wo_sem, x_send, x_recv, wo_send, wo_recv,
    h_send, h_recv, m_send, m_recv, t_send, t_recv, s_send, s_recv, halo_send, halo_recv, ready,
):
    tp = lax.axis_index("tp")
    sp = lax.axis_index("sp")
    rows, depth = tok.shape
    ret_w, att_w, kv_w = rq.shape[1], aq.shape[1], ak.shape[1]
    heads = ld_in.shape[0]
    chunks = rows // CHUNK
    pairs = ret_w // LANES
    att_pairs = att_w // LANES
    att_heads = att_w // HEAD_DIM
    kv_heads = kv_w // HEAD_DIM
    group = att_heads // kv_heads
    out_rows = rows // n_tp
    model = depth * n_tp
    scale = HEAD_DIM ** (-0.5)
    half = rows // 2
    blocks = rows // WINDOW

    c_ak, c_av = 0, kv_w
    c_pairs = 2 * kv_w
    c_aq = c_pairs + 2 * ret_w
    c_rq = c_aq + att_w
    width = c_rq + ret_w
    parts = [(ak, 0, kv_w, c_ak), (av, 0, kv_w, c_av)]
    for p in range(pairs):
        parts.append((rk, p * LANES, LANES, c_pairs + p * 2 * LANES))
        parts.append((rv, p * LANES, LANES, c_pairs + p * 2 * LANES + LANES))
    parts += [(aq, 0, att_w, c_aq), (rq, 0, ret_w, c_rq)]
    pair_tiles = [
        slice(c_pairs + p * 2 * LANES, c_pairs + (p + 1) * 2 * LANES) for p in range(pairs)
    ]
    kv_tile = slice(c_ak, c_pairs)
    query_tiles = [slice(at, at + TILE) for at in range(c_aq, width, TILE)]

    def c_rk(p):
        return slice(c_pairs + p * 2 * LANES, c_pairs + p * 2 * LANES + LANES)

    def c_rv(p):
        return slice(c_pairs + p * 2 * LANES + LANES, c_pairs + (p + 1) * 2 * LANES)

    def load_tokens(i):
        span = pl.ds(i * half, half)
        return pltpu.make_async_copy(tok.at[span, :], xb.at[0, span, :], tok_sem.at[i])

    def load_weight(phase, i):
        owner = lax.rem(tp + phase, n_tp)
        ref, at, size, col = parts[i]
        return pltpu.make_async_copy(
            ref.at[pl.ds(owner * depth, depth), pl.ds(at, size)],
            wb.at[phase, :, pl.ds(col, size)],
            w_sem.at[phase + 1 if phase > 0 or i >= 4 else 0],
        )

    def wait_weights(group):
        cut = c_pairs + 2 * LANES
        ref = wb.at[max(group - 1, 0)]
        if group < 2:
            ref = ref.at[:, pl.ds(0, cut) if group == 0 else pl.ds(cut, width - cut)]
        pltpu.make_async_copy(ref, ref, w_sem.at[group]).wait()

    def load_exit(i):
        ref = (wr, wa)[i]
        return pltpu.make_async_copy(
            ref, wo.at[i, pl.ds(0, ref.shape[0]), :], wo_sem
        )

    def wait_exit():
        ref = wo.at[:, pl.ds(0, ret_w), :]
        pltpu.make_async_copy(ref, ref, wo_sem).wait()

    def all_tokens(q):
        return pltpu.make_async_remote_copy(
            src_ref=xb.at[0], dst_ref=xb.at[n_tp - q],
            send_sem=x_send.at[q - 1], recv_sem=x_recv.at[n_tp - q - 1],
            device_id={"tp": lax.rem(tp + q, n_tp)}, device_id_type=pl.DeviceIdType.MESH,
        )

    def all_exit(q):
        here_ = wo.at[:, pl.ds((n_tp - q) * ret_w, ret_w), :]
        return pltpu.make_async_remote_copy(
            src_ref=here_, dst_ref=here_,
            send_sem=wo_send.at[q - 1], recv_sem=wo_recv.at[n_tp - q - 1, 0],
            device_id={"tp": lax.rem(tp + q, n_tp)}, device_id_type=pl.DeviceIdType.MESH,
        )

    def all_heads(q):
        target = lax.rem(tp + q, n_tp)
        return pltpu.make_async_remote_copy(
            src_ref=hb.at[pl.ds(target * out_rows, out_rows), :],
            dst_ref=hin.at[n_tp - q - 1],
            send_sem=h_send.at[q - 1], recv_sem=h_recv.at[n_tp - q - 1, 0],
            device_id={"tp": target}, device_id_type=pl.DeviceIdType.MESH,
        )

    def send_total(q):
        return pltpu.make_async_remote_copy(
            src_ref=tot, dst_ref=tin.at[q - 1],
            send_sem=t_send.at[q - 1], recv_sem=t_recv.at[q - 1],
            device_id={"sp": lax.rem(sp + q, n_sp)}, device_id_type=pl.DeviceIdType.MESH,
        )

    def all_states(q):
        return pltpu.make_async_remote_copy(
            src_ref=msg, dst_ref=inbox.at[q - 1],
            send_sem=m_send.at[q - 1], recv_sem=m_recv.at[q - 1],
            device_id={"sp": lax.rem(sp + q, n_sp)}, device_id_type=pl.DeviceIdType.MESH,
        )

    def send_tokens(q, i):
        span = pl.ds(i * half, half)
        return pltpu.make_async_remote_copy(
            src_ref=xb.at[0, span, :], dst_ref=xb.at[n_tp - q, span, :],
            send_sem=x_send.at[q - 1], recv_sem=x_recv.at[n_tp - q - 1],
            device_id={"tp": lax.rem(tp + q, n_tp)}, device_id_type=pl.DeviceIdType.MESH,
        )

    def send_squares(q):
        return pltpu.make_async_remote_copy(
            src_ref=sr.at[0], dst_ref=sr.at[n_tp - q],
            send_sem=s_send.at[q - 1], recv_sem=s_recv.at[n_tp - q - 1],
            device_id={"tp": lax.rem(tp + q, n_tp)}, device_id_type=pl.DeviceIdType.MESH,
        )

    def send_exit(q, i, part):
        size = ret_w // PARTS
        span = pl.ds(part * size, size)
        source = (wr, wa)[i].at[span, :] if i == 1 and part < PARTS // 2 else wo.at[i, span, :]
        return pltpu.make_async_remote_copy(
            src_ref=source,
            dst_ref=wo.at[i, pl.ds((n_tp - q) * ret_w + part * size, size), :],
            send_sem=wo_send.at[q - 1], recv_sem=wo_recv.at[n_tp - q - 1, i],
            device_id={"tp": lax.rem(tp + q, n_tp)}, device_id_type=pl.DeviceIdType.MESH,
        )

    def whole_exit(q, i):
        place = wo.at[i, pl.ds((n_tp - q) * ret_w, ret_w), :]
        return pltpu.make_async_remote_copy(
            src_ref=place, dst_ref=place,
            send_sem=wo_send.at[q - 1], recv_sem=wo_recv.at[n_tp - q - 1, i],
            device_id={"tp": lax.rem(tp + q, n_tp)}, device_id_type=pl.DeviceIdType.MESH,
        )

    def send_heads(q, i):
        target = lax.rem(tp + q, n_tp)
        cols = pl.ds(i * ret_w, (ret_w, att_w)[i])
        return pltpu.make_async_remote_copy(
            src_ref=hb.at[pl.ds(target * out_rows, out_rows), cols],
            dst_ref=hin.at[n_tp - q - 1, :, cols],
            send_sem=h_send.at[q - 1], recv_sem=h_recv.at[n_tp - q - 1, i],
            device_id={"tp": target}, device_id_type=pl.DeviceIdType.MESH,
        )

    def send_state(q, p):
        span = pl.ds(p * HEAD_DIM, HEAD_DIM)
        return pltpu.make_async_remote_copy(
            src_ref=msg.at[span, :], dst_ref=inbox.at[q - 1, span, :],
            send_sem=m_send.at[q - 1], recv_sem=m_recv.at[q - 1],
            device_id={"sp": lax.rem(sp + q, n_sp)}, device_id_type=pl.DeviceIdType.MESH,
        )

    def send_halo():
        cols = pl.ds(c_ak, 2 * kv_w)
        return pltpu.make_async_remote_copy(
            src_ref=pb.at[pl.ds(rows, WINDOW), cols],
            dst_ref=halo,
            send_sem=halo_send, recv_sem=halo_recv,
            device_id={"sp": lax.rem(sp + 1, n_sp)}, device_id_type=pl.DeviceIdType.MESH,
        )

    smalls = [
        pltpu.make_async_copy(src, dst, small_sem.at[i])
        for i, (src, dst) in enumerate(
            ((ld_in, ld), (gain_in, gain), (rgain_in, rgain), (sink_in, sink))
        )
    ]
    for copy in smalls:
        copy.start()
    barrier = pltpu.get_barrier_semaphore()
    for q in range(1, n_tp):
        pl.semaphore_signal(
            barrier, inc=1, device_id={"tp": lax.rem(tp + q, n_tp)},
            device_id_type=pl.DeviceIdType.MESH,
        )
    for q in range(1, n_sp):
        @pl.when(sp + q < n_sp)
        def _():
            pl.semaphore_signal(
                barrier, inc=1, device_id={"sp": lax.rem(sp + q, n_sp)},
                device_id_type=pl.DeviceIdType.MESH,
            )
    load_tokens(0).start()
    for i in range(4):
        load_weight(0, i).start()
    load_tokens(1).start()

    lane1 = lax.broadcasted_iota(jnp.int32, (1, LANES), 1)
    first_lanes = lane1 < HEAD_DIM
    half_masks = (
        jnp.where(first_lanes, scale, 0.0).astype(BF16),
        jnp.where(first_lanes, 0.0, scale).astype(BF16),
    )
    lane = lax.broadcasted_iota(jnp.int32, (CHUNK, LANES), 1)
    row = lax.broadcasted_iota(jnp.int32, (CHUNK, LANES), 0)
    same_head = (row < HEAD_DIM) == (lane < HEAD_DIM)
    before = row > lane
    early[...] = jnp.where(before, 1.0, 0.0).astype(BF16)

    pad = cr.shape[1]
    cr[...] = jnp.zeros_like(cr)
    for copy in smalls:
        copy.wait()
    for i in range(4, len(parts)):
        load_weight(0, i).start()
    for p in range(pairs):
        gt[p] = jnp.broadcast_to(
            rgain[p * LANES : (p + 1) * LANES].reshape(1, LANES), (LANES, LANES)
        ).T
    for h in range(heads):
        for c in range(chunks):
            cr[c, h : h + 1, :] = ld[h, :, c * CHUNK : (c + 1) * CHUNK]
    steps = cr[...].reshape(chunks * pad, CHUNK)
    top = steps.astype(BF16)
    rest = steps - top.astype(F32)
    mid = rest.astype(BF16)
    low = (rest - mid.astype(F32)).astype(BF16)
    upto = jnp.where(row <= lane, 1.0, 0.0).astype(BF16)
    sums = jnp.dot(
        jnp.concatenate([top, mid, low], axis=0), upto, preferred_element_type=F32
    )
    n_steps = chunks * pad
    cumulative = sums[:n_steps] + (sums[n_steps : 2 * n_steps] + sums[2 * n_steps :])
    cr[...] = cumulative.reshape(chunks, pad, CHUNK)
    eqr[...] = jnp.exp(cumulative).reshape(chunks, pad, CHUNK)
    ekr[...] = (jnp.exp(cumulative[:, CHUNK - 1 :] - cumulative) * scale).reshape(
        chunks, pad, CHUNK
    )
    filler = jnp.zeros((LANES - n_steps % LANES, CHUNK), F32)
    columns = jnp.concatenate([cumulative, filler], axis=0).T

    def decay(c, h):
        def piece():
            at = c * pad + h
            wide = jnp.broadcast_to(columns[:, at : at + 1], (CHUNK, LANES))
            gap = jnp.where(row <= lane, cr[c, h : h + 1, :] - wide, -jnp.inf)
            dt[c, h // 2, :, (h % 2) * CHUNK : (h % 2 + 1) * CHUNK] = jnp.exp(gap)

        return piece

    def scaled(i):
        def piece():
            span = slice(i * CHUNK, (i + 1) * CHUNK)
            x = xb[0, span, :].astype(F32)
            xb[0, span, :] = (x * gain[tp]).astype(BF16)
            squares = jnp.broadcast_to(
                jnp.sum(x * x, axis=1, keepdims=True), (CHUNK, LANES)
            )
            sq[span, :] = squares

        return piece

    def turn(i):
        def piece():
            sr[0, i : i + 1, :] = sq[i * CHUNK : (i + 1) * CHUNK, :].T[:1]

        return piece

    def invert(i):
        def piece():
            span = slice(i * CHUNK, (i + 1) * CHUNK)
            line = sr[1, i : i + 1, :]
            for phase in range(2, n_tp):
                line = line + sr[phase, i : i + 1, :]
            squares = sq[span, :] + jnp.broadcast_to(line, (LANES, CHUNK)).T
            inv[span, :] = lax.rsqrt(squares / model + EPS)

        return piece

    def project(phase, cols, i=0, parts_of=1):
        def piece():
            size = rows // parts_of
            span = slice(i * size, (i + 1) * size)
            total = jnp.dot(
                xb[phase, span, :], wb[phase, :, cols], preferred_element_type=F32
            )
            if phase > 0:
                total = acc[span, cols] + total
            if phase == n_tp - 1:
                wide = jnp.concatenate([inv[span, :]] * (TILE // LANES), axis=1)
                pb[WINDOW + i * size : WINDOW + (i + 1) * size, cols] = (
                    total * wide
                ).astype(BF16)
            else:
                acc[span, cols] = total

        return piece

    per_half = half // CHUNK
    last = n_tp - 1
    every = [kv_tile] + pair_tiles + query_tiles
    decays = [decay(c, h) for c in range(chunks) for h in range(heads)]
    weave(decays[:heads])
    decays = decays[heads:]
    load_tokens(0).wait()
    weave([scaled(i) for i in range(per_half)])
    pl.semaphore_wait(barrier, n_tp - 1 + sp)
    for q in range(1, n_tp):
        send_tokens(q, 0).start()
    for q in range(1, n_sp):
        @pl.when(sp >= q)
        def _():
            pl.semaphore_signal(
                ready, inc=1, device_id={"sp": lax.rem(sp + n_sp - q, n_sp)},
                device_id_type=pl.DeviceIdType.MESH,
            )
    load_tokens(1).wait()
    wait_weights(0)
    weave(
        [project(0, cols, 0, 2) for cols in every[:2]],
        [scaled(i) for i in range(per_half, chunks)],
    )
    for q in range(1, n_tp):
        send_tokens(q, 1).start()
    cut = len(decays) // len(every)
    weave(
        [project(0, cols, 1, 2) for cols in every[:2]],
        decays[:cut] + [turn(i) for i in range(chunks)],
    )
    for q in range(1, n_tp):
        send_squares(q).start()
    wait_weights(1)
    for phase in range(1, n_tp):
        for i in range(len(parts)):
            load_weight(phase, i).start()
    for i in range(1, -1, -1):
        load_exit(i).start()
    weave([project(0, cols, i, 2) for cols in every[2:] for i in range(2)], decays[cut:])
    for phase in range(1, n_tp):
        wait_weights(phase + 1)
        send_squares(n_tp - phase).wait_recv()
        all_tokens(n_tp - phase).wait_recv()
        if phase < last:
            weave([project(phase, cols) for cols in every])

    def here(c):
        return pl.ds(pl.multiple_of(WINDOW + c * CHUNK, CHUNK), CHUNK)

    def own_state(p):
        def piece(c):
            turned = pb[here(c), c_rv(p)].T
            vt[c, p] = turned
            wide = turned.astype(F32)
            faded = jnp.concatenate(
                [
                    wide[:HEAD_DIM] * ekr[c, 2 * p : 2 * p + 1, :],
                    wide[HEAD_DIM:] * ekr[c, 2 * p + 1 : 2 * p + 2, :],
                ],
                axis=0,
            ).astype(BF16)
            added = jnp.dot(faded, pb[here(c), c_rk(p)], preferred_element_type=F32)
            ub[c, p] = jnp.where(same_head, added, 0.0)

        def pack():
            state = ub[0, p]
            for c in range(1, chunks):
                state = state * fade_row(c, p) + ub[c, p]
            msg[p * HEAD_DIM : (p + 1) * HEAD_DIM, :] = (
                state[:HEAD_DIM] + state[HEAD_DIM:]
            ).astype(BF16)

        return [functools.partial(piece, c) for c in range(chunks)] + [pack]

    def fade_row(c, p):
        ends = [
            jnp.broadcast_to(eqr[c, h : h + 1, CHUNK - 1 :], (1, LANES))
            for h in (2 * p, 2 * p + 1)
        ]
        return jnp.where(first_lanes, ends[0], ends[1])

    totals = jnp.zeros((1, LANES), F32)
    for h in range(heads):
        total = eqr[0, h : h + 1, CHUNK - 1 :]
        for c in range(1, chunks):
            total = total * eqr[c, h : h + 1, CHUNK - 1 :]
        totals = jnp.where(lane1 == h, jnp.broadcast_to(total, (1, LANES)), totals)
    tot[...] = totals

    def send_states(p):
        for q in range(n_sp - 1, 0, -1):
            @pl.when(sp + q < n_sp)
            def _():
                if p == 0:
                    send_total(q).start()
                send_state(q, p).start()

    def double(i):
        def piece():
            span = slice(i * WINDOW, (i + 1) * WINDOW)
            for t in range(kv_w // LANES):
                keys = pb[span, c_ak + t * LANES : c_ak + (t + 1) * LANES]
                swapped = pltpu.roll(keys.astype(F32), HEAD_DIM, 1).astype(BF16)
                values = pb[span, c_av + t * LANES : c_av + (t + 1) * LANES].T
                for e in range(2):
                    g = 2 * t + e
                    kd[g, span, :] = jnp.where(first_lanes == (e == 0), keys, swapped)
                    va[i, g, :HEAD_DIM, :] = values[e * HEAD_DIM : (e + 1) * HEAD_DIM]
                    va[i, g, HEAD_DIM:, :] = jnp.ones((16, WINDOW), BF16)

        return piece

    def halves(cols):
        return [project(last, cols, i, 2) for i in range(2)]

    for q in range(1, n_tp):
        send_exit(q, 1, 0).start()
    weave([invert(i) for i in range(chunks)])
    weave(halves(kv_tile) + halves(pair_tiles[0]))
    @pl.when((sp > 0) & (sp + 1 < n_sp))
    def _():
        pl.semaphore_wait(ready, n_sp - 1 - sp)
        send_halo().start()

    weave(own_state(0))

    @pl.when((sp == 0) & (sp + 1 < n_sp))
    def _():
        pl.semaphore_wait(ready, n_sp - 1 - sp)
        send_halo().start()

    send_states(0)
    for q in range(1, n_tp):
        send_exit(q, 1, 1).start()
    weave(
        [piece for p in range(1, pairs) for piece in halves(pair_tiles[p])],
        [double(i) for i in range(1, blocks + 1)],
    )
    weave(*[own_state(p) for p in range(1, pairs)])
    for p in range(1, pairs):
        send_states(p)
    wait_exit()
    for q in range(1, n_tp):
        for part in range(2, PARTS):
            send_exit(q, 1, part).start()
        send_exit(q, 0, 0).start()
    weave([piece for cols in query_tiles for piece in halves(cols)])

    per_part = blocks // n_tp

    def block(n):
        part = lax.rem(n // per_part + tp + 1, n_tp)
        return part * per_part + (n + 1) % per_part

    def band(n):
        return pl.ds(pl.multiple_of(block(n) * WINDOW, WINDOW), 2 * WINDOW)

    def score(n):
        def piece(g):
            queries = []
            for h in range(g * group, (g + 1) * group):
                at = c_aq + (h // 2) * LANES
                queries.append(pb[here(block(n)), at : at + LANES] * half_masks[h % 2])
            sc[n, :, g * group * WINDOW : (g + 1) * group * WINDOW] = lax.dot_general(
                kd[g, band(n), :], jnp.concatenate(queries, axis=0), NT,
                preferred_element_type=F32,
            )

        return [functools.partial(piece, g) for g in range(kv_heads)]

    def weigh(n):
        def piece(h):
            cols = slice(h * WINDOW, (h + 1) * WINDOW)
            outside = jnp.where((sp == 0) & (block(n) == 0), -jnp.inf, 0.0).astype(F32)
            s = jnp.where(before, sc[n, :WINDOW, cols] + outside, sc[n, WINDOW:, cols])
            sink_h = jnp.full((1, WINDOW), sink[h], F32)
            top = jnp.maximum(jnp.max(s, axis=0, keepdims=True), sink_h)
            dn[n, h : h + 1, :] = jnp.exp(sink_h - top)
            weights = jnp.exp(s - top).astype(BF16)
            older = weights * early[...]
            pw[n, :WINDOW, cols] = older
            pw[n, WINDOW:, cols] = weights - older

        return [functools.partial(piece, h) for h in range(att_heads)]

    def gather(n):
        def piece(g):
            left = jnp.concatenate([va[block(n), g], va[block(n) + 1, g]], axis=1)
            cols = slice(g * group * WINDOW, (g + 1) * group * WINDOW)
            total = jnp.dot(left, pw[n, :, cols], preferred_element_type=F32)
            for j in range(group):
                h = g * group + j
                cols = slice(j * WINDOW, (j + 1) * WINDOW)
                below = total[HEAD_DIM : HEAD_DIM + 1, cols] + dn[n, h : h + 1, :]
                ao[n, h * HEAD_DIM : (h + 1) * HEAD_DIM, :] = (
                    total[:HEAD_DIM, cols] * (1.0 / below)
                ).astype(BF16)

        def place():
            store = pl.ds(pl.multiple_of(block(n) * WINDOW, WINDOW), WINDOW)
            for p in range(att_pairs):
                hb[store, ret_w + p * LANES : ret_w + (p + 1) * LANES] = ao[
                    n, p * LANES : (p + 1) * LANES, :
                ].T

        return [functools.partial(piece, g) for g in range(kv_heads)] + [place]

    def relate(c):
        def piece(p):
            query = pb[here(c), c_rq + p * LANES : c_rq + (p + 1) * LANES]
            queries = jnp.concatenate([query * half_masks[e] for e in range(2)], axis=0)
            rs[c, p] = lax.dot_general(
                pb[here(c), c_rk(p)], queries, NT, preferred_element_type=F32
            )

        return [functools.partial(piece, p) for p in range(pairs)]

    def fade(c):
        def piece(p):
            rw[c, p] = (rs[c, p] * dt[c, p]).astype(BF16)

        return [functools.partial(piece, p) for p in range(pairs)]

    def recall(c):
        def piece(p):
            total = jnp.dot(vt[c, p], rw[c, p], preferred_element_type=F32)
            ri[c, p, :HEAD_DIM, :] = total[:HEAD_DIM, :CHUNK]
            ri[c, p, HEAD_DIM:, :] = total[HEAD_DIM:, CHUNK:]

        return [functools.partial(piece, p) for p in range(pairs)]

    for i in range(blocks + 2):
        if i % per_part == per_part - 1 and i < blocks:
            @pl.when((tp == n_tp - 1 - i // per_part) & (sp > 0))
            def _():
                send_halo().wait_recv()
                pb[:WINDOW, kv_tile] = halo[...]
                double(0)()

            @pl.when((tp == n_tp - 1 - i // per_part) & (sp == 0))
            def _():
                pb[:WINDOW, kv_tile] = jnp.zeros((WINDOW, 2 * kv_w), BF16)
                double(0)()

        first, second, third = (0 <= i - k < blocks for k in range(3))
        weave(
            (score(i) + relate(i) if first else [])
            + (gather(i - 2) + recall(i - 2) if third else []),
            weigh(i - 1) + fade(i - 1) if second else [],
        )
        for q in range(1, n_tp):
            if i - 1 == q * per_part:
                send_heads(q, 1).start()
                for part in range(1, PARTS):
                    send_exit(q, 0, part).start()

    mine = pl.ds(pl.multiple_of(tp * out_rows, out_rows), out_rows)

    def leave(kind, n):
        def piece():
            cols = slice(n * TILE, (n + 1) * TILE)
            inner = slice(kind * ret_w, (kind + 1) * ret_w)
            left = jnp.concatenate(
                [hb[mine, inner]] + [hin[phase - 1, :, inner] for phase in range(1, n_tp)],
                axis=1,
            )
            total = jnp.dot(left, wo[kind, :, cols], preferred_element_type=F32)
            if kind == 1:
                oacc[:, cols] = total
            else:
                out[:, cols] = (oacc[:, cols] + total).astype(BF16)

        return piece

    for phase in range(1, n_tp):
        whole_exit(n_tp - phase, 1).wait_recv()
        send_heads(n_tp - phase, 1).wait_recv()
    exits = [leave(1, n) for n in range(model // TILE)]
    share = len(exits) // 2
    weave(exits[:share])
    st[...] = jnp.zeros_like(st)
    for q in range(n_sp - 1, 0, -1):
        @pl.when(sp >= q)
        def _():
            all_states(q).wait_recv()
            send_total(q).wait_recv()
            tail = tin[q - 1]
            for p in range(pairs):
                part = inbox[q - 1, p * HEAD_DIM : (p + 1) * HEAD_DIM, :].astype(F32)
                fade = jnp.where(
                    first_lanes,
                    jnp.broadcast_to(tail[:, 2 * p : 2 * p + 1], (1, LANES)),
                    jnp.broadcast_to(tail[:, 2 * p + 1 : 2 * p + 2], (1, LANES)),
                )
                both = jnp.concatenate([part, part], axis=0)
                st[p] = st[p] * fade + jnp.where(same_head, both, 0.0)

    for p in range(pairs):
        state = st[p]
        for c in range(chunks):
            stb[c, p] = state.astype(BF16)
            if c + 1 < chunks:
                state = state * fade_row(c, p) + ub[c, p]

    def finish(c):
        def piece(p):
            query = pb[here(c), c_rq + p * LANES : c_rq + (p + 1) * LANES]
            carried = lax.dot_general(stb[c, p], query, NT, preferred_element_type=F32)
            normed = []
            for e in range(2):
                span = slice(e * HEAD_DIM, (e + 1) * HEAD_DIM)
                h = 2 * p + e
                r = ri[c, p, span, :] + carried[span] * eqr[c, h : h + 1, :]
                square = jnp.sum(r * r, axis=0, keepdims=True)
                normed.append(
                    (r * lax.rsqrt(square * (1.0 / HEAD_DIM) + EPS) * gt[p, span, :]).astype(BF16)
                )
            rows_c = pl.ds(pl.multiple_of(c * CHUNK, CHUNK), CHUNK)
            hb[rows_c, p * LANES : (p + 1) * LANES] = jnp.concatenate(normed, axis=0).T

        return [functools.partial(piece, p) for p in range(pairs)]

    each = chunks // n_tp
    for q in range(1, n_tp):
        first = lax.rem(tp + q, n_tp) * each
        weave([piece for i in range(each) for piece in finish(first + i)])
        send_heads(q, 0).start()
    weave(
        [leave(1, n) for n in range(model // TILE)],
        [piece for i in range(each) for piece in finish(tp * each + i)],
    )
    for phase in range(1, n_tp):
        whole_exit(n_tp - phase, 0).wait_recv()
        send_heads(n_tp - phase, 0).wait_recv()
    weave([leave(0, n) for n in range(model // TILE)])
    for q in range(1, n_tp):
        send_squares(q).wait_send()
        all_tokens(q).wait_send()
        all_exit(q).wait_send()
        all_heads(q).wait_send()
    for q in range(1, n_sp):
        @pl.when(sp + q < n_sp)
        def _():
            all_states(q).wait_send()
            send_total(q).wait_send()

    @pl.when(sp + 1 < n_sp)
    def _():
        send_halo().wait_send()


def shards(n_sp, n_tp, tokens, in_gain, rq, rk, rv, aq, ak, av, log_decay, ret_gain, sink, wr, wa):
    rows, depth = tokens.shape[1:]
    ret_w, att_w, kv_w = rq.shape[1], aq.shape[1], ak.shape[1]
    heads = log_decay.shape[1]
    model = depth * n_tp
    width = 3 * ret_w + att_w + 2 * kv_w
    chunks, pairs, blocks = rows // CHUNK, ret_w // LANES, rows // WINDOW
    att_heads = att_w // HEAD_DIM
    out_rows = rows // n_tp
    later = max(n_sp - 1, 1)
    others = max(n_tp - 1, 1)
    packed = pairs * HEAD_DIM
    pad = 8
    hbm = pl.BlockSpec(memory_space=pltpu.HBM)
    dma = pltpu.SemaphoreType.DMA
    result = pl.pallas_call(
        functools.partial(layer, n_sp, n_tp),
        out_shape=pltpu.VMEM((out_rows, model), BF16),
        in_specs=[hbm] * 13,
        out_specs=pl.BlockSpec(memory_space=pltpu.VMEM),
        scratch_shapes=[
            pltpu.VMEM((n_tp, rows, depth), BF16),
            pltpu.VMEM((n_tp, depth, width), BF16),
            pltpu.VMEM((rows, width), F32),
            pltpu.VMEM((WINDOW + rows, width), BF16),
            pltpu.VMEM((rows, LANES), F32),
            pltpu.VMEM((rows, LANES), F32),
            pltpu.VMEM((chunks, pad, CHUNK), F32),
            pltpu.VMEM((chunks, pad, CHUNK), F32),
            pltpu.VMEM((chunks, pad, CHUNK), F32),
            pltpu.VMEM((chunks, pairs, CHUNK, 2 * CHUNK), F32),
            pltpu.VMEM((chunks, pairs, LANES, CHUNK), BF16),
            pltpu.VMEM((chunks, pairs, LANES, LANES), F32),
            pltpu.VMEM((pairs, LANES, LANES), F32),
            pltpu.VMEM((chunks, pairs, LANES, LANES), BF16),
            pltpu.VMEM((chunks, pairs, LANES, CHUNK), F32),
            pltpu.VMEM((WINDOW, WINDOW), BF16),
            pltpu.VMEM((kv_w // HEAD_DIM, WINDOW + rows, LANES), BF16),
            pltpu.VMEM((blocks + 1, kv_w // HEAD_DIM, HEAD_DIM + 16, WINDOW), BF16),
            pltpu.VMEM((blocks, 2 * WINDOW, att_heads * WINDOW), F32),
            pltpu.VMEM((blocks, 2 * WINDOW, att_heads * WINDOW), BF16),
            pltpu.VMEM((blocks, 8, WINDOW), F32),
            pltpu.VMEM((blocks, att_w, WINDOW), BF16),
            pltpu.VMEM((chunks, pairs, CHUNK, 2 * CHUNK), F32),
            pltpu.VMEM((chunks, pairs, CHUNK, 2 * CHUNK), BF16),
            pltpu.VMEM((packed, LANES), BF16),
            pltpu.VMEM((later, packed, LANES), BF16),
            pltpu.VMEM((1, LANES), F32),
            pltpu.VMEM((later, 1, LANES), F32),
            pltpu.VMEM((WINDOW, 2 * kv_w), BF16),
            pltpu.VMEM((n_tp, 8, CHUNK), F32),
            pltpu.VMEM((rows, ret_w + att_w), BF16),
            pltpu.VMEM((others, out_rows, ret_w + att_w), BF16),
            pltpu.VMEM((2, n_tp * ret_w, model), BF16),
            pltpu.VMEM((out_rows, model), F32),
            pltpu.VMEM((pairs, LANES, LANES), F32),
            pltpu.VMEM((n_tp, 1, depth), F32),
            pltpu.VMEM((heads, 1, rows), F32),
            pltpu.VMEM((ret_w,), F32),
            pltpu.SMEM(sink.shape, F32),
            dma((4,)), dma((2,)), dma((n_tp + 1,)), dma,
            dma((others,)), dma((others,)),
            dma((others,)), dma((others, 2)),
            dma((others,)), dma((others, 2)),
            dma((later,)), dma((later,)),
            dma((later,)), dma((later,)),
            dma((others,)), dma((others,)),
            dma, dma, pltpu.SemaphoreType.REGULAR,
        ],
        compiler_params=pltpu.CompilerParams(
            collective_id=0, has_side_effects=True, vmem_limit_bytes=62 * 1024 * 1024
        ),
    )(
        tokens[0], in_gain.reshape(n_tp, 1, depth), rq, rk, rv, aq, ak, av,
        jnp.transpose(log_decay, (1, 0, 2)), ret_gain, sink, wr, wa,
    )
    return result[None]


def solution(mesh):
    n_sp, n_tp = mesh.shape["sp"], mesh.shape["tp"]
    return jax.shard_map(
        functools.partial(shards, n_sp, n_tp),
        mesh=mesh,
        in_specs=(
            P("fs", "sp", "tp"),
            P(),
            P(None, "tp"),
            P(None, "tp"),
            P(None, "tp"),
            P(None, "tp"),
            P(None, "tp"),
            P(None, "tp"),
            P("fs", "tp", "sp"),
            P("tp"),
            P("tp"),
            P("tp", None),
            P("tp", None),
        ),
        out_specs=P("fs", ("sp", "tp"), None),
        check_vma=False,
    )
```
